32 devices in a mesh: sp: 16 (over z, y, x), tp: 2 (over core).
Axes of the slice: x: 2, y: 2, z: 4, core: 2. Of those that a mesh axis runs over, the one named last changes fastest.
Arguments:
- queries: bfloat16 [4096, 1024], P('sp', 'tp'), may hold values from -7 to 7
- keys: bfloat16 [4096, 256], P('sp', 'tp'), may hold values from -6 to 6
- values: bfloat16 [4096, 256], P('sp', 'tp'), may hold values from -6 to 6
- q_gain: float32 [64], replicated, may hold values from 0.5 to 5
- k_gain: float32 [64], replicated, may hold values from 0.5 to 5
- resid: bfloat16 [4096, 2048], P(('sp', 'tp')), may hold values from -6 to 6
- out_weight: bfloat16 [1024, 2048], P('tp'), may hold values from -0.1875 to 0.1875
- post_gain: float32 [2048], replicated, may hold values from 0.1 to 1.9
- ffn_gain: float32 [2048], replicated, may hold values from 0.1 to 1.9
- post_ffn_gain: float32 [2048], replicated, may hold values from 0.1 to 1.9
- gate_w: bfloat16 [16, 2048, 3584], P('sp', None, 'tp'), may hold values from -0.125 to 0.125
- up_w: bfloat16 [16, 2048, 3584], P('sp', None, 'tp'), may hold values from -0.125 to 0.125
- down_w: bfloat16 [16, 3584, 2048], P('sp', 'tp'), may hold values from -0.09375 to 0.09375
- route_ids: int32 [4096, 2], P(('sp', 'tp')), may hold values from 0 to 15, all different within a row; in each aligned block of 128 rows (0 to 127, 128 to 255, ...) at most 24 rows name the same one
- route_w: float32 [4096, 2], P(('sp', 'tp')), may hold values from 0.2 to 1
Outputs:
- layer_out: bfloat16 [4096, 2048], P(('sp', 'tp'))
The draws below stay inside these ranges and needn't reach their ends.
Inputs may be any that keep to these rules, and one draw needn't show every extreme that they name: `route_ids`: each row names 2 different experts. In each aligned block of 128 rows (the rows of one device) no expert is named more than 24 times, a bound that some blocks reach.
All inputs are finite; a program needn't handle non-finite values.
Results may differ from the reference program's by a relative error of at most 0.017.
The reference program's roundings to bfloat16 on the way count: a program that leaves them out, or rounds other values in their place, can miss the bound.
Values may be sent and summed in bfloat16 or wider, within the bound.
No kernel may reach another device: no remote copies, remote signals or barrier semaphores. Data moves between devices by JAX's collectives and lax.ppermute only.
A program may use at most 128 MiB of HBM per device.

```python
import math
import jax
import jax.numpy as jnp
import numpy as np
from jax import lax

D = 2048
HEADS = 16
KV_HEADS = 4
HEAD_DIM = 64
FF_E = 3584
GRID_W = 64
TOP = 2
TOKENS = 4096
EXPERTS = 16
ROWS_DEV = 128
CAP = 24
N_SP = 16
N_TP = 2


def base_keys(key):
    fresh = jax.random.normal(jax.random.fold_in(key, 11), (TOKENS, KV_HEADS * HEAD_DIM), jnp.float32)
    return jnp.clip(fresh, -6.0, 6.0)


def draw_keys(key, part):
    return base_keys(key).astype(jnp.bfloat16)


def draw_queries(key, part):
    fresh = jax.random.normal(jax.random.fold_in(key, 12), (TOKENS, HEADS, HEAD_DIM), jnp.float32)
    fresh = jnp.clip(fresh, -6.0, 6.0)
    return fresh.reshape(TOKENS, HEADS * HEAD_DIM).astype(jnp.bfloat16)


def gain_draw(key, salt):
    spread = jax.random.uniform(jax.random.fold_in(key, salt), (HEAD_DIM,), jnp.float32, math.log(0.5), math.log(2.0))
    return jnp.exp(spread)


def draw_q_gain(key, part):
    return gain_draw(key, 13)


def draw_k_gain(key, part):
    return gain_draw(key, 14)


def levels(stream_key, extent, shards, smallest, largest):
    factor_of, own = 1.0, jax.random.fold_in(stream_key, 6)
    for position, blocks in shards:
        heights = jnp.exp(jax.random.uniform(jax.random.fold_in(own, position), (blocks,), jnp.float32, smallest / len(shards), largest / len(shards)))
        factor_of = factor_of * jnp.repeat(heights, extent[position] // blocks).reshape([-1 if axis == position else 1 for axis in range(len(extent))])
    return factor_of


def routed_block(rng, own, number, rows, count, top, reach, skew):
    ranking = jax.random.permutation(rng, count)
    heavy_load, common = portions_of(count, rows * top, reach, skew, True), portions_of(count, rows * top, reach, skew, False)
    places = jnp.arange(count)

    def named(lengths, turn):
        used = int((lengths > 0).sum())
        fixed = max(1, used // 4)
        shifted = fixed + (places - fixed + turn * (used - fixed)) % max(1, count - fixed)
        return jnp.zeros((count,), jnp.int32).at[ranking[jnp.where(places < fixed, places, shifted)]].set(jnp.asarray(lengths, jnp.int32))

    lengths = jnp.where(number % 4 == 0, named(heavy_load, number // 4), named(common, number - number // 4 - 1))
    mixed = jax.random.permutation(jax.random.fold_in(own, 3), count)
    source_of, receiver = mixed[0:count // 2 * 2:2], mixed[1:count // 2 * 2:2]
    slack = jnp.minimum(lengths[source_of] - 1, reach - lengths[receiver]) // 2
    slack = jnp.where((source_of == ranking[0]) | (receiver == ranking[0]) | (lengths[receiver] == 0), 0, jnp.maximum(slack, 0))
    shifted = jax.random.randint(jax.random.fold_in(own, 4), (count // 2,), 0, 1 << 20) % (slack + 1)
    lengths = lengths.at[source_of].add(-shifted).at[receiver].add(shifted)
    labels = jnp.searchsorted(jnp.cumsum(lengths), jnp.arange(rows * top), side="right").astype(jnp.int32)
    listing = labels.reshape(top, rows).T
    listing = listing[jax.random.permutation(jax.random.fold_in(own, 1), rows)]
    turn = jax.random.randint(jax.random.fold_in(own, 2), (rows, 1), 0, top)
    return jnp.take_along_axis(listing, (jnp.arange(top)[None, :] + turn) % top, axis=1)


def portions_of(amount, total, limit, slope, full):
    loads = [(1 << 20) // math.isqrt(standing ** slope) + 1 for standing in range(1, amount + 1)]
    largest = limit if full else min(limit, max(-(-total // amount), total * loads[0] // sum(loads)))
    least = 1 if total - largest >= amount - 1 else 0
    holding, rest = [largest] + [least] * (amount - 1), total - largest - least * (amount - 1)
    while rest > 0:
        candidates = [i for i in range(1, amount) if holding[i] < largest] or [i for i in range(1, amount) if holding[i] < limit]
        mass, remaining = sum([loads[i] for i in candidates]), rest
        for i in candidates:
            addition = min(limit - holding[i], max(1, remaining * loads[i] // mass), rest)
            holding[i] = holding[i] + addition
            rest = rest - addition
    return np.array(holding)


def noise(key, shape, deviation, most, cuts=(), held_as=jnp.bfloat16):
    array = jax.random.normal(key, shape, jnp.float32) * deviation
    if len(cuts) > 0:
        array = levels(key, shape, cuts, -0.22, 0.18) * array
    return jnp.clip(array, min=-most, max=most).astype(held_as)


def setup_inputs(seed: int = 0) -> dict:
    streams_of = jax.random.split(jax.random.key(seed), 16)
    queries = draw_queries(jax.random.fold_in(streams_of[15], 71), 0)
    keys = draw_keys(jax.random.fold_in(streams_of[15], 71), 0)
    values = noise(streams_of[2], (TOKENS, KV_HEADS * HEAD_DIM), 1.0, 6.0, ((0, 16), (1, 2)))
    q_gain = draw_q_gain(jax.random.fold_in(streams_of[15], 71), 0)
    k_gain = draw_k_gain(jax.random.fold_in(streams_of[15], 71), 0)
    resid = noise(streams_of[5], (TOKENS, D), 1.0, 6.0, ((0, 32),))
    out_weight = noise(streams_of[6], (HEADS * HEAD_DIM, D), (HEADS * HEAD_DIM) ** -0.5, 0.1875, ((0, 2),))
    post_gain = jnp.clip(1.0 + 0.18 * jax.random.normal(streams_of[7], (D,), jnp.float32), 0.1, 1.9)
    ffn_gain = jnp.clip(1.0 + 0.18 * jax.random.normal(streams_of[8], (D,), jnp.float32), 0.1, 1.9)
    post_ffn_gain = jnp.clip(1.0 + 0.18 * jax.random.normal(streams_of[9], (D,), jnp.float32), 0.1, 1.9)
    gate_w = noise(streams_of[10], (EXPERTS, D, FF_E), D ** -0.5, 0.125, ((0, 16), (2, 2)))
    up_w = noise(streams_of[11], (EXPERTS, D, FF_E), D ** -0.5, 0.125, ((0, 16), (2, 2)))
    down_w = noise(streams_of[12], (EXPERTS, FF_E, D), FF_E ** -0.5, 0.09375, ((0, 16), (1, 2)))
    route_ids_keys = jax.random.split(jax.random.fold_in(streams_of[13], 1), TOKENS // ROWS_DEV)
    route_ids_turns = jax.random.permutation(jax.random.fold_in(streams_of[13], 3), TOKENS // ROWS_DEV)
    route_ids = jax.vmap(lambda own, number: routed_block(jax.random.fold_in(streams_of[13], 2), own, number, ROWS_DEV, EXPERTS, TOP, CAP, 1))(route_ids_keys, route_ids_turns).reshape((TOKENS, TOP))
    route_w = jnp.clip(0.2 + 0.8 * jax.random.uniform(streams_of[14], (TOKENS, TOP), jnp.float32) ** levels(streams_of[14], (TOKENS, TOP), ((0, 32),), -0.2, 0.2), 0.2, 1.0)
    return dict(queries=queries, keys=keys, values=values, q_gain=q_gain, k_gain=k_gain, resid=resid, out_weight=out_weight, post_gain=post_gain, ffn_gain=ffn_gain, post_ffn_gain=post_ffn_gain, gate_w=gate_w, up_w=up_w, down_w=down_w, route_ids=route_ids, route_w=route_w)


EPS = 1e-06
THETA = 10000.0

def qk_prepare(raw, gain, positions, head_count):
    count_rows = raw.shape[0]
    values32 = raw.astype(jnp.float32).reshape(count_rows, head_count, HEAD_DIM)
    normed = values32 * lax.rsqrt(lax.optimization_barrier(jnp.mean(values32 * values32, axis=-1, keepdims=True)) + EPS) * gain
    half_dim = HEAD_DIM // 2
    freqs = THETA ** (-jnp.arange(0, half_dim, 2, dtype=jnp.float32) / half_dim)
    grid_row = (positions // GRID_W).astype(jnp.float32)
    grid_col = (positions % GRID_W).astype(jnp.float32)
    angles = jnp.concatenate([grid_row[:, None] * freqs, grid_col[:, None] * freqs], axis=-1)
    cosine = jnp.cos(angles)[:, None, :]
    sine = jnp.sin(angles)[:, None, :]
    paired = normed.reshape(count_rows, head_count, half_dim, 2)
    first = paired[..., 0]
    second = paired[..., 1]
    turned = jnp.stack([first * cosine - second * sine, first * sine + second * cosine], axis=-1)
    return turned.reshape(count_rows, head_count * HEAD_DIM).astype(jnp.bfloat16)

def rms_scale(values32, gain):
    return values32 * lax.rsqrt(lax.optimization_barrier(jnp.mean(values32 * values32, axis=-1, keepdims=True)) + EPS) * gain

def reference(queries, keys, values, q_gain, k_gain, resid, out_weight, post_gain, ffn_gain, post_ffn_gain, gate_w, up_w, down_w, route_ids, route_w):
    positions = jnp.arange(TOKENS, dtype=jnp.int32)
    group_size = HEADS // KV_HEADS
    scale_factor = HEAD_DIM ** (-0.5)
    query_n = qk_prepare(queries, q_gain, positions, HEADS).reshape(TOKENS // 128, 128, KV_HEADS, group_size, HEAD_DIM)
    key_n = qk_prepare(keys, k_gain, positions, KV_HEADS).reshape(TOKENS, KV_HEADS, HEAD_DIM).astype(jnp.float32)
    value_n = values.reshape(TOKENS, KV_HEADS, HEAD_DIM).astype(jnp.float32)

    def attend(block):
        scores = jnp.einsum('qhgd,khd->hgqk', block.astype(jnp.float32), key_n) * scale_factor
        top_score = lax.optimization_barrier(jnp.max(scores, axis=-1, keepdims=True))
        expo = jnp.exp(scores - top_score)
        total = lax.optimization_barrier(jnp.sum(expo, axis=-1))
        weights = lax.optimization_barrier(expo.astype(jnp.bfloat16)).astype(jnp.float32)
        summed = jnp.einsum('hgqk,khd->qhgd', weights, value_n)
        result = summed / jnp.transpose(total, (2, 0, 1))[..., None]
        return result.astype(jnp.bfloat16).reshape(128, HEADS * HEAD_DIM)
    attended = lax.map(attend, query_n).reshape(TOKENS, HEADS * HEAD_DIM)
    mixed = jnp.dot(attended, out_weight, preferred_element_type=jnp.float32)
    hidden_state = (resid.astype(jnp.float32) + rms_scale(mixed, post_gain)).astype(jnp.bfloat16)
    normed = rms_scale(hidden_state.astype(jnp.float32), ffn_gain).astype(jnp.bfloat16)
    bound = CAP * N_SP * N_TP
    pair_count = TOKENS * TOP
    pair_experts = route_ids.reshape(-1)
    padded_rows = jnp.concatenate([normed, jnp.zeros((1, D), jnp.bfloat16)], axis=0)
    part_width = FF_E // N_TP

    def expert_pass(expert):
        slots = jnp.nonzero(pair_experts == expert, size=bound, fill_value=pair_count)[0].astype(jnp.int32)
        token_ids = jnp.where(slots < pair_count, slots // TOP, TOKENS).astype(jnp.int32)
        rows_in = padded_rows[token_ids]
        gate = jnp.dot(rows_in, gate_w[expert], preferred_element_type=jnp.float32)
        upward = jnp.dot(rows_in, up_w[expert], preferred_element_type=jnp.float32)
        inner = (jax.nn.silu(gate) * upward).astype(jnp.bfloat16)
        down_here = down_w[expert]
        total = jnp.zeros((bound, D), jnp.float32)
        for part in range(N_TP):
            partial_sum = jnp.dot(inner[:, part * part_width:(part + 1) * part_width], down_here[part * part_width:(part + 1) * part_width], preferred_element_type=jnp.float32)
            total = total + lax.optimization_barrier(partial_sum.astype(jnp.bfloat16)).astype(jnp.float32)
        return (slots, total.astype(jnp.bfloat16))
    slot_table, results = lax.map(expert_pass, jnp.arange(EXPERTS, dtype=jnp.int32))
    placed = jnp.zeros((pair_count + 1, D), jnp.bfloat16).at[slot_table.reshape(-1)].set(results.reshape(-1, D))
    picked = placed[:pair_count].reshape(TOKENS, TOP, D).astype(jnp.float32)
    combined = lax.optimization_barrier(jnp.sum(route_w[:, :, None] * picked, axis=1))
    return (hidden_state.astype(jnp.float32) + rms_scale(combined, post_ffn_gain)).astype(jnp.bfloat16)
```

```python
import functools

import jax
import jax.numpy as jnp
from jax import lax
from jax.experimental import pallas as pl
from jax.experimental.pallas import tpu as pltpu
from jax.sharding import PartitionSpec as P

HEAD_DIM = 64
GRID_W = 64
LANES = 128
EPS = 1e-06
THETA = 10000.0
VMEM_BYTES = 56 * 1024 * 1024
F32 = jnp.float32
BF16 = jnp.bfloat16


def dot(a, b):
    return jnp.dot(a, b, preferred_element_type=F32)


def dot_t(a, b):
    return lax.dot_general(a, b, (((1,), (1,)), ((), ())), preferred_element_type=F32)


def params():
    return pltpu.CompilerParams(vmem_limit_bytes=VMEM_BYTES)


def prep_kernel(q_ref, k_ref, v_ref, cos_ref, sin_ref, qg_ref, qgs_ref, kg_ref, kgs_ref, qn_ref, kv_ref):
    tok = q_ref.shape[0]
    row = lax.broadcasted_iota(jnp.int32, (LANES, LANES), 0)
    col = lax.broadcasted_iota(jnp.int32, (LANES, LANES), 1)
    swap = jnp.where(row == (col ^ 1), 1.0, 0.0).astype(BF16)
    mean = jnp.where((row // HEAD_DIM) == (col // HEAD_DIM), 1.0 / HEAD_DIM, 0.0).astype(BF16)
    lane = lax.broadcasted_iota(jnp.int32, (tok, LANES), 1)
    cos = cos_ref[...]
    sin = sin_ref[...]

    def turn(x, gain, gain_swapped):
        x32 = x.astype(F32)
        square = x32 * x32
        high = square.astype(BF16)
        low = (square - high.astype(F32)).astype(BF16)
        scale = lax.rsqrt(dot(high, mean) + dot(low, mean) + EPS)
        return (x32 * (cos * gain) + dot(x, swap) * (sin * gain_swapped)) * scale

    kv_ref[:, :LANES] = turn(k_ref[...], kg_ref[...], kgs_ref[...]).astype(BF16)
    kv_ref[:, LANES:] = v_ref[...]
    heads = q_ref.shape[1] // HEAD_DIM
    group = heads // 2
    for pair in range(heads // 2):
        out = turn(q_ref[:, pair * LANES:(pair + 1) * LANES], qg_ref[...], qgs_ref[...]) * (HEAD_DIM ** -0.5)
        rolled = pltpu.roll(out, HEAD_DIM, 1)
        for side in range(2):
            head = 2 * pair + side
            kv = head // group
            source = out if side == kv else rolled
            qn_ref[head] = jnp.where((lane // HEAD_DIM) == kv, source, 0.0).astype(BF16)


def prep(queries, keys, values, q_gain, k_gain):
    tok = queries.shape[0]
    heads = queries.shape[1] // HEAD_DIM
    positions = lax.axis_index("sp") * tok + jnp.arange(tok, dtype=jnp.int32)[:, None]
    lane = jnp.arange(LANES, dtype=jnp.int32)[None, :]
    half = HEAD_DIM // 2
    freqs = THETA ** (-((lane % half) // 2 * 2).astype(F32) / half)
    place = jnp.where(lane % HEAD_DIM < half, positions // GRID_W, positions % GRID_W)
    angles = place.astype(F32) * freqs
    cos = jnp.cos(angles)
    sin = jnp.sin(angles) * jnp.where(lane % 2 == 0, -1.0, 1.0)

    def gains(gain):
        both = jnp.tile(gain, 2)
        return both[None, :], both.reshape(-1, 2)[:, ::-1].reshape(1, -1)

    return pl.pallas_call(
        prep_kernel,
        out_shape=(
            jax.ShapeDtypeStruct((heads, tok, LANES), BF16),
            jax.ShapeDtypeStruct((tok, 2 * LANES), BF16),
        ),
        compiler_params=params(),
        name="prep",
    )(queries, keys, values, cos, sin, *gains(q_gain), *gains(k_gain))


def attend_kernel(*refs, counts, first, last, heads_step):
    q_ref = refs[0]
    n = len(counts)
    kv_refs = refs[1:1 + n]
    at = 1 + n
    if not first:
        m_in, acc_in = refs[at:at + 2]
        at += 2
    if last:
        out_ref = refs[at]
        at += 1
    else:
        m_out, acc_out = refs[at:at + 2]
        at += 2
    vaug = refs[at]
    tok = q_ref.shape[1]
    step = pl.program_id(0)

    blocks = []
    for ref, count in zip(kv_refs, counts):
        for c in range(count):
            blocks.append((ref, c * tok))

    @pl.when(step == 0)
    def _():
        for b, (ref, at_row) in enumerate(blocks):
            vaug[b * tok:(b + 1) * tok, :LANES] = ref[at_row:at_row + tok, LANES:]
            vaug[b * tok:(b + 1) * tok, LANES:] = jnp.ones((tok, LANES), BF16)

    outs = []
    for h in range(heads_step):
        q = q_ref[h]
        scores = [dot_t(q, ref[at_row:at_row + tok, :LANES]) for ref, at_row in blocks]
        top = scores[0]
        for s in scores[1:]:
            top = jnp.maximum(top, s)
        m = jnp.max(top, axis=1, keepdims=True)
        if not first:
            before = m_in[h][:, :1]
            m = jnp.maximum(m, before)
        weights = jnp.concatenate([jnp.exp(s - m).astype(BF16) for s in scores], axis=1)
        acc = dot(weights, vaug[...])
        if not first:
            acc = acc + acc_in[h] * jnp.exp(before - m)
        if last:
            outs.append(acc[:, :LANES] / acc[:, LANES:])
        else:
            m_out[h] = jnp.broadcast_to(m, (tok, LANES))
            acc_out[h] = acc
    if last:
        lane = lax.broadcasted_iota(jnp.int32, (tok, LANES), 1)
        group_steps = pl.num_programs(0) // 2
        kv = step // group_steps
        for pair in range(heads_step // 2):
            a, b = outs[2 * pair], outs[2 * pair + 1]
            low = jnp.where(lane < HEAD_DIM, a, pltpu.roll(b, HEAD_DIM, 1))
            high = jnp.where(lane < HEAD_DIM, pltpu.roll(a, HEAD_DIM, 1), b)
            out_ref[:, pair * LANES:(pair + 1) * LANES] = jnp.where(kv == 0, low, high).astype(BF16)


def attend(qn, kv_list, carry, last, heads_step=2):
    heads, tok, _ = qn.shape
    counts = tuple(kv.shape[0] // tok for kv in kv_list)
    first = carry is None
    whole = lambda shape: pl.BlockSpec(shape, lambda i: (0,) * len(shape))
    head_spec = lambda width: pl.BlockSpec((heads_step, tok, width), lambda i: (i, 0, 0))
    in_specs = [head_spec(LANES)] + [whole(kv.shape) for kv in kv_list]
    args = [qn, *kv_list]
    if not first:
        in_specs += [head_spec(LANES), head_spec(2 * LANES)]
        args += list(carry)
    if last:
        out_shape = jax.ShapeDtypeStruct((tok, heads * HEAD_DIM), BF16)
        out_specs = pl.BlockSpec((tok, heads_step * HEAD_DIM), lambda i: (0, i))
    else:
        out_shape = (
            jax.ShapeDtypeStruct((heads, tok, LANES), F32),
            jax.ShapeDtypeStruct((heads, tok, 2 * LANES), F32),
        )
        out_specs = (head_spec(LANES), head_spec(2 * LANES))
    total = sum(counts) * tok
    return pl.pallas_call(
        functools.partial(attend_kernel, counts=counts, first=first, last=last, heads_step=heads_step),
        grid=(heads // heads_step,),
        in_specs=in_specs,
        out_specs=out_specs,
        out_shape=out_shape,
        scratch_shapes=[pltpu.VMEM((total, 2 * LANES), BF16)],
        compiler_params=params(),
        cost_estimate=pl.CostEstimate(
            flops=4 * heads * tok * total * 256, bytes_accessed=total * 512, transcendentals=heads * tok * total
        ),
        name="attend",
    )(*args)


def rms(x, gain):
    return x * lax.rsqrt(jnp.mean(x * x, axis=-1, keepdims=True) + EPS) * gain


def project_kernel(own_ref, other_ref, w_own, w_other, resid_ref, pg_ref, fg_ref, slot_ref, hidden_ref, out_ref):
    mixed = dot(own_ref[...], w_own[...]) + dot(other_ref[...], w_other[...])
    hidden = (resid_ref[...].astype(F32) + rms(mixed, pg_ref[...])).astype(BF16)
    hidden_ref[...] = hidden
    normed = rms(hidden.astype(F32), fg_ref[...]).astype(BF16)
    slots, rows = out_ref.shape[0], hidden.shape[0]
    number = lax.broadcasted_iota(jnp.int32, (slots, rows), 0)
    chosen = number == slot_ref[0:1, :]
    for k in range(1, slot_ref.shape[0]):
        chosen = chosen | (number == slot_ref[k:k + 1, :])
    out_ref[...] = dot(jnp.where(chosen, 1.0, 0.0).astype(BF16), normed).astype(BF16)


def project(own, other, w_own, w_other, resid, post_gain, ffn_gain, slot_rows, slots):
    rows, width = resid.shape
    return pl.pallas_call(
        project_kernel,
        out_shape=(
            jax.ShapeDtypeStruct((rows, width), BF16),
            jax.ShapeDtypeStruct((slots, width), BF16),
        ),
        compiler_params=params(),
        name="project",
    )(own, other, w_own, w_other, resid, post_gain[None, :], ffn_gain[None, :], slot_rows)


def expert_kernel(own_ref, other_ref, gate_ref, up_ref, down_ref, y_own, y_other, x_ref, acc_ref):
    step = pl.program_id(0)
    rows = own_ref.shape[0]

    @pl.when(step == 0)
    def _():
        x_ref[:rows] = own_ref[...]
        x_ref[rows:] = other_ref[...]

    x = x_ref[...]
    gate = dot(x, gate_ref[0])
    up = dot(x, up_ref[0])
    inner = (gate / (1.0 + jnp.exp(-gate)) * up).astype(BF16)
    part = dot(inner, down_ref[0])

    @pl.when(step == 0)
    def _():
        acc_ref[...] = part

    @pl.when(step > 0)
    def _():
        acc_ref[...] += part

    @pl.when(step == pl.num_programs(0) - 1)
    def _():
        y_own[...] = acc_ref[:rows].astype(BF16)
        y_other[...] = acc_ref[rows:].astype(BF16)


def expert(own, other, gate_w, up_w, down_w):
    rows, width = own.shape
    hidden = gate_w.shape[2]
    block = 256 if hidden % 256 == 0 else 128
    whole = pl.BlockSpec((rows, width), lambda i: (0, 0))
    return pl.pallas_call(
        expert_kernel,
        grid=(hidden // block,),
        in_specs=[
            whole,
            whole,
            pl.BlockSpec((1, width, block), lambda i: (0, 0, i)),
            pl.BlockSpec((1, width, block), lambda i: (0, 0, i)),
            pl.BlockSpec((1, block, width), lambda i: (0, i, 0)),
        ],
        out_specs=(whole, whole),
        out_shape=(jax.ShapeDtypeStruct((rows, width), BF16),) * 2,
        scratch_shapes=[pltpu.VMEM((2 * rows, width), BF16), pltpu.VMEM((2 * rows, width), F32)],
        compiler_params=params(),
        name="expert",
    )(own, other, gate_w, up_w, down_w)


def combine_kernel(back_ref, slot_ref, weight_ref, hidden_ref, gain_ref, out_ref):
    slots, rows = back_ref.shape[0], hidden_ref.shape[0]
    number = lax.broadcasted_iota(jnp.int32, (rows, slots), 1)
    combined = None
    for k in range(slot_ref.shape[1]):
        pick = jnp.where(number == slot_ref[:, k:k + 1], 1.0, 0.0).astype(BF16)
        part = dot(pick, back_ref[...]) * weight_ref[:, k:k + 1]
        combined = part if combined is None else combined + part
    out_ref[...] = (hidden_ref[...].astype(F32) + rms(combined, gain_ref[...])).astype(BF16)


def combine(back, slot_ids, route_w, hidden, gain):
    return pl.pallas_call(
        combine_kernel,
        out_shape=jax.ShapeDtypeStruct(hidden.shape, BF16),
        compiler_params=params(),
        name="combine",
    )(back, slot_ids, route_w, hidden, gain[None, :])


def swap_tp(x):
    count = lax.axis_size("tp")
    return lax.ppermute(x, "tp", [(i, (i + 1) % count) for i in range(count)])


def move(x, perm):
    return lax.ppermute(x, "sp", perm)


def per_device(
    queries,
    keys,
    values,
    q_gain,
    k_gain,
    resid,
    out_weight,
    post_gain,
    ffn_gain,
    post_ffn_gain,
    gate_w,
    up_w,
    down_w,
    route_ids,
    route_w,
):
    tok_local = queries.shape[0]
    width = resid.shape[1]
    tp_count = lax.axis_size("tp")
    sp_count = lax.axis_size("sp")
    row_count = tok_local // tp_count

    qn, kv = prep(queries, keys, values, q_gain, k_gain)

    far = 4
    plane = sp_count // far
    own = [kv]
    z_blocks = [
        move(kv, [(i, (i // plane ^ d) * plane + i % plane) for i in range(sp_count)]) for d in range(1, far)
    ]
    near = [move(kv, [(i, i ^ d) for i in range(sp_count)]) for d in range(1, plane)]
    stacked = jnp.concatenate(z_blocks, axis=0)
    beyond = [move(stacked, [(i, i ^ d) for i in range(sp_count)]) for d in range(1, plane)]
    w_other = swap_tp(out_weight)

    carry = attend(qn, own + z_blocks + near, None, False)
    attended = attend(qn, beyond, carry, True)

    attended = attended.reshape(tp_count, row_count, attended.shape[1])
    tp_index = lax.axis_index("tp")
    heads_own = lax.dynamic_index_in_dim(attended, tp_index, 0, False)
    heads_other = swap_tp(lax.dynamic_index_in_dim(attended, (tp_index + 1) % tp_count, 0, False))

    top_count = route_ids.shape[1]
    expert_count = gate_w.shape[0] * sp_count
    capacity = 3 * tok_local * top_count // (2 * tp_count * expert_count)
    slots = expert_count * capacity
    flat_routes = route_ids.reshape(-1)
    chosen = (flat_routes[:, None] == jnp.arange(expert_count, dtype=jnp.int32)[None, :]).astype(jnp.int32)
    earlier = jnp.cumsum(chosen, axis=0) - chosen
    ranks = jnp.sum(earlier * chosen, axis=1)
    slot_ids = (flat_routes * capacity + ranks).reshape(row_count, top_count)

    hidden, outgoing = project(
        heads_own, heads_other, out_weight, w_other, resid, post_gain, ffn_gain, slot_ids.T, slots
    )
    arrived = lax.all_to_all(
        outgoing.reshape(expert_count, capacity, width), "sp", split_axis=0, concat_axis=0, tiled=True
    ).reshape(slots, width)
    y_own, y_other = expert(arrived, swap_tp(arrived), gate_w, up_w, down_w)
    expert_out = (y_own.astype(F32) + swap_tp(y_other).astype(F32)).astype(BF16)
    returned = lax.all_to_all(
        expert_out.reshape(expert_count, capacity, width), "sp", split_axis=0, concat_axis=0, tiled=True
    ).reshape(slots, width)
    return combine(returned, slot_ids, route_w, hidden, post_ffn_gain)


def solution(mesh):
    in_specs = (
        P("sp", "tp"),
        P("sp", "tp"),
        P("sp", "tp"),
        P(),
        P(),
        P(("sp", "tp"), None),
        P("tp", None),
        P(),
        P(),
        P(),
        P("sp", None, "tp"),
        P("sp", None, "tp"),
        P("sp", "tp", None),
        P(("sp", "tp"), None),
        P(("sp", "tp"), None),
    )
    out_specs = P(("sp", "tp"), None)
    return jax.shard_map(
        per_device, mesh=mesh, in_specs=in_specs, out_specs=out_specs, check_vma=False
    )
```

```python
import functools

import jax
import jax.numpy as jnp
import numpy as np
from jax import lax
from jax.experimental import pallas as pl
from jax.experimental.pallas import tpu as pltpu
from jax.sharding import PartitionSpec as P

HEAD_DIM = 64
GRID_W = 64
LANES = 128
EPS = 1e-06
THETA = 10000.0
MIB = 1024 * 1024
F32 = jnp.float32
BF16 = jnp.bfloat16


def dot(a, b):
    return jnp.dot(a, b, preferred_element_type=F32)


def dot_t(a, b):
    return lax.dot_general(a, b, (((1,), (1,)), ((), ())), preferred_element_type=F32)


def params(mib):
    return pltpu.CompilerParams(vmem_limit_bytes=mib * MIB)


def prep_kernel(base_ref, q_ref, k_ref, v_ref, freq_ref, qg_ref, kg_ref, qn_ref, kv_ref):
    tok = q_ref.shape[0]
    grid_rows = tok // GRID_W
    row = lax.broadcasted_iota(jnp.int32, (LANES, LANES), 0)
    col = lax.broadcasted_iota(jnp.int32, (LANES, LANES), 1)
    swap = jnp.where(row == (col ^ 1), 1.0, 0.0).astype(BF16)
    mean = jnp.where((row // HEAD_DIM) == (col // HEAD_DIM), 1.0 / HEAD_DIM, 0.0).astype(BF16)
    lane = lax.broadcasted_iota(jnp.int32, (tok, LANES), 1)

    def angles(first, count):
        place = first + lax.broadcasted_iota(jnp.int32, (count, LANES), 0)
        return place.astype(F32) * freq_ref[...]

    sign = jnp.where(lax.broadcasted_iota(jnp.int32, (1, LANES), 1) % 2 == 0, -1.0, 1.0)
    by_row = angles(base_ref[0] // GRID_W, max(8, grid_rows))
    by_col = angles(0, GRID_W)
    row_lanes = lax.broadcasted_iota(jnp.int32, (GRID_W, LANES), 1) % HEAD_DIM < HEAD_DIM // 2

    def spread(rows, cols):
        parts = [
            jnp.where(row_lanes, jnp.broadcast_to(rows[i:i + 1], (GRID_W, LANES)), cols) for i in range(grid_rows)
        ]
        return jnp.concatenate(parts, axis=0)

    cos = spread(jnp.cos(by_row), jnp.cos(by_col))
    sin = spread(jnp.sin(by_row) * sign, jnp.sin(by_col) * sign)

    def factors(gain_ref):
        gain = jnp.broadcast_to(jnp.concatenate([gain_ref[...]] * 2, axis=1), (8, LANES))
        even = lax.broadcasted_iota(jnp.int32, (8, LANES), 1) % 2 == 0
        swapped = jnp.where(even, pltpu.roll(gain, LANES - 1, 1), pltpu.roll(gain, 1, 1))
        return cos * gain[:1], sin * swapped[:1]

    def turn(x, cos_gain, sin_gain):
        x32 = x.astype(F32)
        square = x32 * x32
        high = square.astype(BF16)
        low = (square - high.astype(F32)).astype(BF16)
        scale = lax.rsqrt(dot(high, mean) + dot(low, mean) + EPS)
        return (x32 * cos_gain + dot(x, swap) * sin_gain) * scale

    kv_ref[:, :LANES] = turn(k_ref[...], *factors(kg_ref)).astype(BF16)
    kv_ref[:, LANES:] = v_ref[...]
    heads = q_ref.shape[1] // HEAD_DIM
    group = heads // 2
    q_factors = factors(qg_ref)
    for pair in range(heads // 2):
        out = turn(q_ref[:, pair * LANES:(pair + 1) * LANES], *q_factors) * (HEAD_DIM ** -0.5)
        rolled = pltpu.roll(out, HEAD_DIM, 1)
        for side in range(2):
            head = 2 * pair + side
            kv = head // group
            source = out if side == kv else rolled
            qn_ref[head] = jnp.where((lane // HEAD_DIM) == kv, source, 0.0).astype(BF16)


def prep(queries, keys, values, q_gain, k_gain):
    tok = queries.shape[0]
    heads = queries.shape[1] // HEAD_DIM
    base = (lax.axis_index("sp") * tok).astype(jnp.int32).reshape(1)
    half = HEAD_DIM // 2
    freqs = (THETA ** (-((np.arange(LANES) % half) // 2 * 2) / half)).astype(np.float32)[None, :]
    vmem = pl.BlockSpec(memory_space=pltpu.VMEM)
    return pl.pallas_call(
        prep_kernel,
        in_specs=[pl.BlockSpec(memory_space=pltpu.SMEM)] + [vmem] * 6,
        out_specs=(vmem, vmem),
        out_shape=(
            jax.ShapeDtypeStruct((heads, tok, LANES), BF16),
            jax.ShapeDtypeStruct((tok, 2 * LANES), BF16),
        ),
        compiler_params=params(56),
        name="prep",
    )(base, queries, keys, values, jnp.asarray(freqs), q_gain[None, :], k_gain[None, :])


def route_kernel(self_ref, ids_ref, pick_ref, pack_ref, *, experts, capacity):
    rows, top = ids_ref.shape
    slots = experts * capacity
    lane = lax.broadcasted_iota(jnp.int32, (rows, experts), 1)
    chosen = [jnp.where(ids_ref[:, k:k + 1] == lane, 1.0, 0.0) for k in range(top)]
    both = chosen[0]
    for c in chosen[1:]:
        both = both + c
    row = lax.broadcasted_iota(jnp.int32, (rows, rows), 0)
    col = lax.broadcasted_iota(jnp.int32, (rows, rows), 1)
    earlier = dot(jnp.where(col < row, 1.0, 0.0).astype(BF16), both.astype(BF16))
    number = lax.broadcasted_iota(jnp.int32, (rows, slots), 1)
    packed = None
    for k in range(top):
        rank = jnp.sum(earlier * chosen[k], axis=1, keepdims=True).astype(jnp.int32)
        place = ids_ref[:, k:k + 1] ^ self_ref[0]
        pick = jnp.where(number == place * capacity + rank, 1.0, 0.0)
        pick_ref[k] = pick.astype(BF16)
        packed = pick if packed is None else packed + pick
    unit = jnp.where(row == col, 1.0, 0.0).astype(BF16)
    pack_ref[...] = lax.dot_general(
        packed.astype(BF16), unit, (((0,), (0,)), ((), ())), preferred_element_type=F32
    ).astype(BF16)


def route(route_ids, own_place, experts, capacity):
    rows, top = route_ids.shape
    vmem = pl.BlockSpec(memory_space=pltpu.VMEM)
    return pl.pallas_call(
        functools.partial(route_kernel, experts=experts, capacity=capacity),
        in_specs=[pl.BlockSpec(memory_space=pltpu.SMEM), vmem],
        out_specs=(vmem, vmem),
        out_shape=(
            jax.ShapeDtypeStruct((top, rows, experts * capacity), BF16),
            jax.ShapeDtypeStruct((experts * capacity, rows), BF16),
        ),
        compiler_params=params(16),
        name="route",
    )(own_place.astype(jnp.int32).reshape(1), route_ids)


def attend_kernel(*refs, counts, first, last, heads_step):
    q_ref = refs[0]
    n = len(counts)
    kv_refs = refs[1:1 + n]
    at = 1 + n
    if not first:
        m_in, acc_in = refs[at:at + 2]
        at += 2
    if last:
        out_ref = refs[at]
        at += 1
    else:
        m_out, acc_out = refs[at:at + 2]
        at += 2
    vaug = refs[at]
    tok = q_ref.shape[1]
    step = pl.program_id(0)

    blocks = []
    for ref, count in zip(kv_refs, counts):
        for c in range(count):
            blocks.append((ref, c * tok))

    @pl.when(step == 0)
    def _():
        for b, (ref, at_row) in enumerate(blocks):
            vaug[b * tok:(b + 1) * tok, :LANES] = ref[at_row:at_row + tok, LANES:]
            vaug[b * tok:(b + 1) * tok, LANES:] = jnp.ones((tok, LANES), BF16)

    outs = []
    for h in range(heads_step):
        q = q_ref[h]
        scores = [dot_t(q, ref[at_row:at_row + tok, :LANES]) for ref, at_row in blocks]
        top = scores[0]
        for s in scores[1:]:
            top = jnp.maximum(top, s)
        m = jnp.max(top, axis=1, keepdims=True)
        if not first:
            before = m_in[h][:, :1]
            m = jnp.maximum(m, before)
        weights = jnp.concatenate([jnp.exp(s - m).astype(BF16) for s in scores], axis=1)
        acc = dot(weights, vaug[...])
        if not first:
            acc = acc + acc_in[h] * jnp.exp(before - m)
        if last:
            outs.append(acc[:, :LANES] / acc[:, LANES:])
        else:
            m_out[h] = jnp.broadcast_to(m, (tok, LANES))
            acc_out[h] = acc
    if last:
        lane = lax.broadcasted_iota(jnp.int32, (tok, LANES), 1)
        group_steps = pl.num_programs(0) // 2
        kv = step // group_steps
        for pair in range(heads_step // 2):
            a, b = outs[2 * pair], outs[2 * pair + 1]
            low = jnp.where(lane < HEAD_DIM, a, pltpu.roll(b, HEAD_DIM, 1))
            high = jnp.where(lane < HEAD_DIM, pltpu.roll(a, HEAD_DIM, 1), b)
            out_ref[:, pair * LANES:(pair + 1) * LANES] = jnp.where(kv == 0, low, high).astype(BF16)


def attend(qn, kv_list, carry, last, heads_step=4):
    heads, tok, _ = qn.shape
    counts = tuple(kv.shape[0] // tok for kv in kv_list)
    first = carry is None
    whole = lambda shape: pl.BlockSpec(shape, lambda i: (0,) * len(shape))
    head_spec = lambda width: pl.BlockSpec((heads_step, tok, width), lambda i: (i, 0, 0))
    in_specs = [head_spec(LANES)] + [whole(kv.shape) for kv in kv_list]
    args = [qn, *kv_list]
    if not first:
        in_specs += [head_spec(LANES), head_spec(2 * LANES)]
        args += list(carry)
    if last:
        out_shape = jax.ShapeDtypeStruct((tok, heads * HEAD_DIM), BF16)
        out_specs = pl.BlockSpec((tok, heads_step * HEAD_DIM), lambda i: (0, i))
    else:
        out_shape = (
            jax.ShapeDtypeStruct((heads, tok, LANES), F32),
            jax.ShapeDtypeStruct((heads, tok, 2 * LANES), F32),
        )
        out_specs = (head_spec(LANES), head_spec(2 * LANES))
    total = sum(counts) * tok
    return pl.pallas_call(
        functools.partial(attend_kernel, counts=counts, first=first, last=last, heads_step=heads_step),
        grid=(heads // heads_step,),
        in_specs=in_specs,
        out_specs=out_specs,
        out_shape=out_shape,
        scratch_shapes=[pltpu.VMEM((total, 2 * LANES), BF16)],
        compiler_params=params(28),
        cost_estimate=pl.CostEstimate(
            flops=4 * heads * tok * total * 256, bytes_accessed=total * 512, transcendentals=heads * tok * total
        ),
        name="attend",
    )(*args)


def rms(x, gain):
    return x * lax.rsqrt(jnp.mean(x * x, axis=-1, keepdims=True) + EPS) * gain


def project_kernel(
    tp_ref,
    own_ref,
    other_hbm,
    w_own_hbm,
    w_other_hbm,
    resid_hbm,
    pg_ref,
    fg_ref,
    pack_ref,
    hidden_ref,
    *refs,
    pieces,
):
    out_refs, refs = refs[:pieces], refs[pieces:]
    other_ref, w_own, w_other, resid_ref, sem = refs
    rows = resid_ref.shape[0]
    mine = pl.ds(pl.multiple_of(tp_ref[0] * rows, rows), rows)
    copies = (
        pltpu.make_async_copy(w_own_hbm, w_own, sem.at[0]),
        pltpu.make_async_copy(other_hbm.at[mine, :], other_ref, sem.at[1]),
        pltpu.make_async_copy(w_other_hbm, w_other, sem.at[2]),
        pltpu.make_async_copy(resid_hbm, resid_ref, sem.at[3]),
    )
    for copy in copies:
        copy.start()
    copies[0].wait()
    mixed = dot(own_ref[mine, :], w_own[...])
    copies[1].wait()
    copies[2].wait()
    mixed = mixed + dot(other_ref[...], w_other[...])
    copies[3].wait()
    hidden = (resid_ref[...].astype(F32) + rms(mixed, pg_ref[...])).astype(BF16)
    hidden_ref[...] = hidden
    normed = rms(hidden.astype(F32), fg_ref[...]).astype(BF16)
    count = out_refs[0].shape[0]
    for n, ref in enumerate(out_refs):
        ref[...] = dot(pack_ref[n * count:(n + 1) * count, :], normed).astype(BF16)


def project(own, other, w_own, w_other, resid, post_gain, ffn_gain, pack, pieces):
    rows, width = resid.shape
    count = pack.shape[0] // pieces
    tp_index = lax.axis_index("tp").astype(jnp.int32).reshape(1)
    vmem = pl.BlockSpec(memory_space=pltpu.VMEM)
    hbm = pl.BlockSpec(memory_space=pltpu.HBM)
    return pl.pallas_call(
        functools.partial(project_kernel, pieces=pieces),
        in_specs=[pl.BlockSpec(memory_space=pltpu.SMEM), vmem, hbm, hbm, hbm, hbm, vmem, vmem, vmem],
        out_specs=(vmem,) * (1 + pieces),
        out_shape=(jax.ShapeDtypeStruct((rows, width), BF16),)
        + (jax.ShapeDtypeStruct((count, width), BF16),) * pieces,
        scratch_shapes=[
            pltpu.VMEM((rows, own.shape[1]), BF16),
            pltpu.VMEM(w_own.shape, BF16),
            pltpu.VMEM(w_own.shape, BF16),
            pltpu.VMEM((rows, width), BF16),
            pltpu.SemaphoreType.DMA((4,)),
        ],
        compiler_params=params(24),
        name="project",
    )(tp_index, own, other, w_own, w_other, resid, post_gain[None, :], ffn_gain[None, :], pack)


def expert_kernel(*refs, pieces, block, out_block):
    x_refs, refs = refs[:pieces], refs[pieces:]
    gate_hbm, up_hbm, down_hbm, refs = refs[0:2], refs[2:4], refs[4:6], refs[6:]
    y_refs, refs = refs[:pieces], refs[pieces:]
    x_ref, inner_ref, gate_ref, up_ref, down_ref, rise_sem, fall_sem = refs
    width, hidden = gate_ref.shape[1:]
    steps, falls = hidden // block, width // out_block
    count = x_refs[0].shape[0]

    def rise_copies(half, i):
        at = pl.ds(pl.multiple_of(i * block, block), block)
        return (
            pltpu.make_async_copy(gate_hbm[half].at[0, :, at], gate_ref.at[half, :, at], rise_sem.at[half, 0, i]),
            pltpu.make_async_copy(up_hbm[half].at[0, :, at], up_ref.at[half, :, at], rise_sem.at[half, 1, i]),
        )

    def fall_copies(i):
        at = pl.ds(pl.multiple_of(i * out_block, out_block), out_block)
        return tuple(
            pltpu.make_async_copy(down_hbm[half].at[0, :, at], down_ref.at[half, :, at], fall_sem.at[half, i])
            for half in range(2)
        )

    for half in range(2):
        for i in range(steps):
            for copy in rise_copies(half, i):
                copy.start()
    for i in range(falls):
        for copy in fall_copies(i):
            copy.start()
    for n, ref in enumerate(x_refs):
        x_ref[n * count:(n + 1) * count, :] = ref[...]

    for half in range(2):

        def rise(i, carry, half=half):
            for copy in rise_copies(half, i):
                copy.wait()
            at = pl.ds(pl.multiple_of(i * block, block), block)
            x = x_ref[...]
            gate = dot(x, gate_ref[half, :, at])
            up = dot(x, up_ref[half, :, at])
            inner_ref[half, :, at] = (gate / (1.0 + jnp.exp(-gate)) * up).astype(BF16)
            return carry

        lax.fori_loop(0, steps, rise, 0)

    def fall(i, carry):
        for copy in fall_copies(i):
            copy.wait()
        at = pl.ds(pl.multiple_of(i * out_block, out_block), out_block)
        total = None
        for half in range(2):
            part = dot(inner_ref[half], down_ref[half, :, at]).astype(BF16).astype(F32)
            total = part if total is None else total + part
        total = total.astype(BF16)
        for n, ref in enumerate(y_refs):
            ref[:, at] = total[n * count:(n + 1) * count, :]
        return carry

    lax.fori_loop(0, falls, fall, 0)


def expert(pieces, gate_w, up_w, down_w):
    count, width = pieces[0].shape
    rows = count * len(pieces)
    hidden = gate_w[0].shape[2]
    block = 256 if hidden % 256 == 0 else 128
    out_block = 512 if width % 512 == 0 else 128
    vmem = pl.BlockSpec(memory_space=pltpu.VMEM)
    hbm = pl.BlockSpec(memory_space=pltpu.HBM)
    return pl.pallas_call(
        functools.partial(expert_kernel, pieces=len(pieces), block=block, out_block=out_block),
        in_specs=[vmem] * len(pieces) + [hbm] * 6,
        out_specs=(vmem,) * len(pieces),
        out_shape=(jax.ShapeDtypeStruct((count, width), BF16),) * len(pieces),
        scratch_shapes=[
            pltpu.VMEM((rows, width), BF16),
            pltpu.VMEM((2, rows, hidden), BF16),
            pltpu.VMEM((2, width, hidden), BF16),
            pltpu.VMEM((2, width, hidden), BF16),
            pltpu.VMEM((2, hidden, width), BF16),
            pltpu.SemaphoreType.DMA((2, 2, hidden // block)),
            pltpu.SemaphoreType.DMA((2, width // out_block)),
        ],
        compiler_params=params(54),
        cost_estimate=pl.CostEstimate(
            flops=12 * rows * width * hidden, bytes_accessed=12 * width * hidden, transcendentals=2 * rows * hidden
        ),
        name="expert",
    )(*pieces, *gate_w, *up_w, *down_w)


def combine_kernel(*refs, pieces):
    back_refs, refs = refs[:pieces], refs[pieces:]
    pick_ref, weight_ref, hidden_ref, gain_ref, out_ref, back_ref = refs
    count = back_refs[0].shape[0]
    for n, ref in enumerate(back_refs):
        back_ref[n * count:(n + 1) * count, :] = ref[...]
    combined = None
    for k in range(pick_ref.shape[0]):
        part = dot(pick_ref[k], back_ref[...]) * weight_ref[:, k:k + 1]
        combined = part if combined is None else combined + part
    out_ref[...] = (hidden_ref[...].astype(F32) + rms(combined, gain_ref[...])).astype(BF16)


def combine(back, pick, route_w, hidden, gain):
    return pl.pallas_call(
        functools.partial(combine_kernel, pieces=len(back)),
        out_shape=jax.ShapeDtypeStruct(hidden.shape, BF16),
        scratch_shapes=[pltpu.VMEM((pick.shape[2], hidden.shape[1]), BF16)],
        compiler_params=params(16),
        name="combine",
    )(*back, pick, route_w, hidden, gain[None, :])


def swap_tp(x):
    count = lax.axis_size("tp")
    return lax.ppermute(x, "tp", [(i, (i + 1) % count) for i in range(count)])


def move(x, perm):
    return lax.ppermute(x, "sp", perm)


def per_device(
    queries,
    keys,
    values,
    q_gain,
    k_gain,
    resid,
    out_weight,
    post_gain,
    ffn_gain,
    post_ffn_gain,
    gate_w,
    up_w,
    down_w,
    route_ids,
    route_w,
):
    tok_local = queries.shape[0]
    width = resid.shape[1]
    tp_count = lax.axis_size("tp")
    sp_count = lax.axis_size("sp")
    top_count = route_ids.shape[1]
    expert_count = gate_w.shape[0] * sp_count
    capacity = 3 * tok_local * top_count // (2 * tp_count * expert_count)
    slots = expert_count * capacity

    qn, kv = prep(queries, keys, values, q_gain, k_gain)

    far = 4
    plane = sp_count // far
    own = [kv]
    z_blocks = [
        move(kv, [(i, (i // plane ^ d) * plane + i % plane) for i in range(sp_count)]) for d in range(1, far)
    ]
    near = [move(kv, [(i, i ^ d) for i in range(sp_count)]) for d in range(1, plane)]
    stacked = jnp.concatenate(z_blocks, axis=0)
    beyond = [move(stacked, [(i, i ^ d) for i in range(sp_count)]) for d in range(1, plane)]
    w_other = swap_tp(out_weight)
    gates = (gate_w, swap_tp(gate_w))
    ups = (up_w, swap_tp(up_w))
    downs = (down_w, swap_tp(down_w))
    exchange = sp_count <= 0 and capacity % 8 == 0 and expert_count == sp_count
    own_place = lax.axis_index("sp") if exchange else jnp.zeros((), jnp.int32)
    pick, pack = route(route_ids, own_place, expert_count, capacity)

    carry = attend(qn, own + z_blocks + near, None, False)
    attended = attend(qn, beyond, carry, True)
    hidden, *outgoing = project(
        attended,
        swap_tp(attended),
        out_weight,
        w_other,
        resid,
        post_gain,
        ffn_gain,
        pack,
        expert_count if exchange else 1,
    )
    if exchange:
        groups = ([], [])
        for d in range(sp_count):
            groups[d // 2 % 2].append(d)
        groups = [sorted(g, reverse=True) for g in groups]
        far_move = lambda x, d: x if d == 0 else move(x, [(i, i ^ d) for i in range(sp_count)])
        arrived = [[far_move(outgoing[d], d) for d in g] for g in groups]
        returned = [None] * sp_count
        for g, pieces in zip(groups, arrived):
            done = expert(pieces, gates, ups, downs)
            for d, piece in zip(g, done):
                returned[d] = far_move(piece, d)
    else:
        swap_all = lambda x: lax.all_to_all(
            x.reshape(expert_count, capacity, width), "sp", split_axis=0, concat_axis=0, tiled=True
        ).reshape(slots, width)
        returned = [swap_all(expert([swap_all(outgoing[0])], gates, ups, downs)[0])]
    return combine(returned, pick, route_w, hidden, post_ffn_gain)


def solution(mesh):
    in_specs = (
        P("sp", "tp"),
        P("sp", "tp"),
        P("sp", "tp"),
        P(),
        P(),
        P(("sp", "tp"), None),
        P("tp", None),
        P(),
        P(),
        P(),
        P("sp", None, "tp"),
        P("sp", None, "tp"),
        P("sp", "tp", None),
        P(("sp", "tp"), None),
        P(("sp", "tp"), None),
    )
    out_specs = P(("sp", "tp"), None)
    return jax.shard_map(
        per_device, mesh=mesh, in_specs=in_specs, out_specs=out_specs, check_vma=False
    )
```

```python
import functools

import jax
import jax.numpy as jnp
import numpy as np
from jax import lax
from jax.experimental import pallas as pl
from jax.experimental.pallas import tpu as pltpu
from jax.sharding import PartitionSpec as P


HEAD_DIM = 64
GRID_W = 64
LANES = 128
EPS = 1e-06
THETA = 10000.0
MIB = 1024 * 1024
F32 = jnp.float32
BF16 = jnp.bfloat16


def dot(a, b):
    return jnp.dot(a, b, preferred_element_type=F32)


def dot_t(a, b):
    return lax.dot_general(a, b, (((1,), (1,)), ((), ())), preferred_element_type=F32)


def params(mib):
    return pltpu.CompilerParams(vmem_limit_bytes=mib * MIB)


def prep_kernel(base_ref, q_ref, k_ref, v_ref, freq_ref, qg_ref, kg_ref, qn_ref, kv_ref):
    tok = q_ref.shape[0]
    grid_rows = tok // GRID_W
    row = lax.broadcasted_iota(jnp.int32, (LANES, LANES), 0)
    col = lax.broadcasted_iota(jnp.int32, (LANES, LANES), 1)
    swap = jnp.where(row == (col ^ 1), 1.0, 0.0).astype(BF16)
    mean = jnp.where((row // HEAD_DIM) == (col // HEAD_DIM), 1.0 / HEAD_DIM, 0.0).astype(BF16)
    lane = lax.broadcasted_iota(jnp.int32, (tok, LANES), 1)

    def angles(first, count):
        place = first + lax.broadcasted_iota(jnp.int32, (count, LANES), 0)
        return place.astype(F32) * freq_ref[...]

    sign = jnp.where(lax.broadcasted_iota(jnp.int32, (1, LANES), 1) % 2 == 0, -1.0, 1.0)
    by_row = angles(base_ref[0] // GRID_W, max(8, grid_rows))
    by_col = angles(0, GRID_W)
    row_lanes = lax.broadcasted_iota(jnp.int32, (GRID_W, LANES), 1) % HEAD_DIM < HEAD_DIM // 2

    def spread(rows, cols):
        parts = [
            jnp.where(row_lanes, jnp.broadcast_to(rows[i:i + 1], (GRID_W, LANES)), cols) for i in range(grid_rows)
        ]
        return jnp.concatenate(parts, axis=0)

    cos = spread(jnp.cos(by_row), jnp.cos(by_col))
    sin = spread(jnp.sin(by_row) * sign, jnp.sin(by_col) * sign)

    def factors(gain_ref):
        gain = jnp.broadcast_to(jnp.concatenate([gain_ref[...]] * 2, axis=1), (8, LANES))
        even = lax.broadcasted_iota(jnp.int32, (8, LANES), 1) % 2 == 0
        swapped = jnp.where(even, pltpu.roll(gain, LANES - 1, 1), pltpu.roll(gain, 1, 1))
        return cos * gain[:1], sin * swapped[:1]

    def turn(x, cos_gain, sin_gain):
        x32 = x.astype(F32)
        square = x32 * x32
        high = square.astype(BF16)
        low = (square - high.astype(F32)).astype(BF16)
        scale = lax.rsqrt(dot(high, mean) + dot(low, mean) + EPS)
        return (x32 * cos_gain + dot(x, swap) * sin_gain) * scale

    kv_ref[:, :LANES] = turn(k_ref[...], *factors(kg_ref)).astype(BF16)
    kv_ref[:, LANES:] = v_ref[...]
    heads = q_ref.shape[1] // HEAD_DIM
    group = heads // 2
    q_factors = factors(qg_ref)
    for pair in range(heads // 2):
        out = turn(q_ref[:, pair * LANES:(pair + 1) * LANES], *q_factors) * (HEAD_DIM ** -0.5)
        rolled = pltpu.roll(out, HEAD_DIM, 1)
        for side in range(2):
            head = 2 * pair + side
            kv = head // group
            source = out if side == kv else rolled
            qn_ref[head] = jnp.where((lane // HEAD_DIM) == kv, source, 0.0).astype(BF16)


def prep(queries, keys, values, q_gain, k_gain):
    tok = queries.shape[0]
    heads = queries.shape[1] // HEAD_DIM
    base = (lax.axis_index("sp") * tok).astype(jnp.int32).reshape(1)
    half = HEAD_DIM // 2
    freqs = (THETA ** (-((np.arange(LANES) % half) // 2 * 2) / half)).astype(np.float32)[None, :]
    vmem = pl.BlockSpec(memory_space=pltpu.VMEM)
    return pl.pallas_call(
        prep_kernel,
        in_specs=[pl.BlockSpec(memory_space=pltpu.SMEM)] + [vmem] * 6,
        out_specs=(vmem, vmem),
        out_shape=(
            pltpu.VMEM((heads, tok, LANES), BF16),
            pltpu.VMEM((tok, 2 * LANES), BF16),
        ),
        compiler_params=params(56),
        name="prep",
    )(base, queries, keys, values, jnp.asarray(freqs), q_gain[None, :], k_gain[None, :])


def route_kernel(place_ref, *refs, sources, top, experts, capacity):
    meta_refs, (pick_ref, weight_ref, pack_ref) = refs[:2 * sources], refs[2 * sources:]
    block = meta_refs[0].shape[1]
    rows, slots = sources * block, pack_ref.shape[0]
    flat = jnp.concatenate([ref[...].astype(F32) for ref in meta_refs], axis=0)
    flat = jnp.concatenate([flat] * (8 // flat.shape[0]), axis=0).T
    stack = lambda first: [
        jnp.concatenate([flat[:, first + s * top + k:first + s * top + k + 1] for s in range(sources)], axis=0)
        for k in range(top)
    ]
    ids = [column.astype(jnp.int32) for column in stack(0)]
    weight_ref[...] = jnp.concatenate(stack(sources * top), axis=1)
    lane = lax.broadcasted_iota(jnp.int32, (rows, experts), 1)
    chosen = [jnp.where(e == lane, 1.0, 0.0) for e in ids]
    both = chosen[0]
    for c in chosen[1:]:
        both = both + c
    row = lax.broadcasted_iota(jnp.int32, (rows, rows), 0)
    col = lax.broadcasted_iota(jnp.int32, (rows, rows), 1)
    before = (col < row) & (col // block == row // block)
    earlier = dot(jnp.where(before, 1.0, 0.0).astype(BF16), both.astype(BF16))
    number = lax.broadcasted_iota(jnp.int32, (rows, slots), 1)
    source = lax.broadcasted_iota(jnp.int32, (rows, 1), 0) // block
    packed = None
    for k in range(top):
        rank = jnp.sum(earlier * chosen[k], axis=1, keepdims=True).astype(jnp.int32)
        if sources == 2:
            mask = ids[k] ^ place_ref[0]
            slot = ((mask // 2) * 2 + source) * capacity + rank
            slot = jnp.where(mask % 2 == place_ref[1], slot, -1)
        else:
            slot = ids[k] * capacity + rank
        pick = jnp.where(number == slot, 1.0, 0.0)
        pick_ref[k] = pick.astype(BF16)
        packed = pick if packed is None else packed + pick
    unit = jnp.where(row == col, 1.0, 0.0).astype(BF16)
    pack_ref[...] = lax.dot_general(
        packed.astype(BF16), unit, (((0,), (0,)), ((), ())), preferred_element_type=F32
    ).astype(BF16)


def route(metas, place, experts, capacity):
    top, block = metas[0].shape
    sources = len(metas) // 2
    rows, slots = sources * block, experts * capacity
    vmem = pl.BlockSpec(memory_space=pltpu.VMEM)
    return pl.pallas_call(
        functools.partial(route_kernel, sources=sources, top=top, experts=experts, capacity=capacity),
        in_specs=[pl.BlockSpec(memory_space=pltpu.SMEM)] + [vmem] * len(metas),
        out_specs=(vmem,) * 3,
        out_shape=(
            jax.ShapeDtypeStruct((top, rows, slots), BF16),
            jax.ShapeDtypeStruct((rows, top), F32),
            jax.ShapeDtypeStruct((slots, rows), BF16),
        ),
        compiler_params=params(16),
        name="route",
    )(place, *metas)


def attend_kernel(*refs, counts, first, last, heads_step):
    q_ref = refs[0]
    n = len(counts)
    kv_refs = refs[1:1 + n]
    at = 1 + n
    if not first:
        m_in, acc_in = refs[at:at + 2]
        at += 2
    if last:
        out_ref = refs[at]
        at += 1
    else:
        m_out, acc_out = refs[at:at + 2]
        at += 2
    vaug = refs[at]
    tok = q_ref.shape[1]
    step = pl.program_id(0)

    blocks = []
    for ref, count in zip(kv_refs, counts):
        for c in range(count):
            blocks.append((ref, c * tok))

    @pl.when(step == 0)
    def _():
        for b, (ref, at_row) in enumerate(blocks):
            vaug[b * tok:(b + 1) * tok, :LANES] = ref[at_row:at_row + tok, LANES:]
            vaug[b * tok:(b + 1) * tok, LANES:] = jnp.ones((tok, LANES), BF16)

    outs = []
    for h in range(heads_step):
        q = q_ref[h]
        scores = [dot_t(q, ref[at_row:at_row + tok, :LANES]) for ref, at_row in blocks]
        top = scores[0]
        for s in scores[1:]:
            top = jnp.maximum(top, s)
        m = jnp.max(top, axis=1, keepdims=True)
        if not first:
            before = m_in[h][:, :1]
            m = jnp.maximum(m, before)
        weights = jnp.concatenate([jnp.exp(s - m).astype(BF16) for s in scores], axis=1)
        acc = dot(weights, vaug[...])
        if not first:
            acc = acc + acc_in[h] * jnp.exp(before - m)
        if last:
            outs.append(acc[:, :LANES] / acc[:, LANES:])
        else:
            m_out[h] = jnp.broadcast_to(m, (tok, LANES))
            acc_out[h] = acc
    if last:
        lane = lax.broadcasted_iota(jnp.int32, (tok, LANES), 1)
        group_steps = pl.num_programs(0) // 2
        kv = step // group_steps
        for pair in range(heads_step // 2):
            a, b = outs[2 * pair], outs[2 * pair + 1]
            low = jnp.where(lane < HEAD_DIM, a, pltpu.roll(b, HEAD_DIM, 1))
            high = jnp.where(lane < HEAD_DIM, pltpu.roll(a, HEAD_DIM, 1), b)
            out_ref[:, pair * LANES:(pair + 1) * LANES] = jnp.where(kv == 0, low, high).astype(BF16)


def attend(qn, kv_list, carry, last, heads_step=4):
    heads, tok, _ = qn.shape
    counts = tuple(kv.shape[0] // tok for kv in kv_list)
    first = carry is None
    whole = lambda shape: pl.BlockSpec(shape, lambda i: (0,) * len(shape))
    head_spec = lambda width: pl.BlockSpec((heads_step, tok, width), lambda i: (i, 0, 0))
    in_specs = [head_spec(LANES)] + [whole(kv.shape) for kv in kv_list]
    args = [qn, *kv_list]
    if not first:
        in_specs += [head_spec(LANES), head_spec(2 * LANES)]
        args += list(carry)
    if last:
        out_shape = jax.ShapeDtypeStruct((tok, heads * HEAD_DIM), BF16)
        out_specs = pl.BlockSpec((tok, heads_step * HEAD_DIM), lambda i: (0, i))
    else:
        out_shape = (
            jax.ShapeDtypeStruct((heads, tok, LANES), F32),
            jax.ShapeDtypeStruct((heads, tok, 2 * LANES), F32),
        )
        out_specs = (head_spec(LANES), head_spec(2 * LANES))
    total = sum(counts) * tok
    return pl.pallas_call(
        functools.partial(attend_kernel, counts=counts, first=first, last=last, heads_step=heads_step),
        grid=(heads // heads_step,),
        in_specs=in_specs,
        out_specs=out_specs,
        out_shape=out_shape,
        scratch_shapes=[pltpu.VMEM((total, 2 * LANES), BF16)],
        compiler_params=params(28),
        cost_estimate=pl.CostEstimate(
            flops=4 * heads * tok * total * 256, bytes_accessed=total * 512, transcendentals=heads * tok * total
        ),
        name="attend",
    )(*args)


def rms(x, gain):
    return x * lax.rsqrt(jnp.mean(x * x, axis=-1, keepdims=True) + EPS) * gain


def project_kernel(tp_ref, own_ref, other_ref, w_own, w_other, *refs, sources):
    resid_refs, refs = refs[:sources], refs[sources:]
    pg_ref, fg_ref, pack_ref, hidden_ref, *out_refs = refs
    rows = hidden_ref.shape[0]
    order = (tp_ref[0], 1 - tp_ref[0])[:sources]

    def spans(ref):
        return jnp.concatenate([ref[pl.ds(pl.multiple_of(t * rows, rows), rows), :] for t in order], axis=0)

    resid = jnp.concatenate([ref[...] for ref in resid_refs], axis=0).astype(F32)
    mixed = dot(spans(own_ref), w_own[...]) + dot(spans(other_ref), w_other[...])
    hidden = (resid + rms(mixed, pg_ref[...])).astype(BF16)
    hidden_ref[...] = hidden[:rows]
    normed = rms(hidden.astype(F32), fg_ref[...]).astype(BF16)
    count = out_refs[0].shape[0]
    for n, ref in enumerate(out_refs):
        ref[...] = dot(pack_ref[n * count:(n + 1) * count, :], normed).astype(BF16)


def project(tp_index, own, other, w_own, w_other, resids, post_gain, ffn_gain, pack, pieces):
    rows, width = resids[0].shape
    count = pack.shape[0] // pieces
    vmem = pl.BlockSpec(memory_space=pltpu.VMEM)
    return pl.pallas_call(
        functools.partial(project_kernel, sources=len(resids)),
        in_specs=[pl.BlockSpec(memory_space=pltpu.SMEM)] + [vmem] * (7 + len(resids)),
        out_specs=(vmem,) * (1 + pieces),
        out_shape=(jax.ShapeDtypeStruct((rows, width), BF16),)
        + (jax.ShapeDtypeStruct((count, width), BF16),) * pieces,
        compiler_params=params(24),
        name="project",
    )(tp_index, own, other, w_own, w_other, *resids, post_gain[None, :], ffn_gain[None, :], pack)


def load_kernel(after_ref, *refs):
    count = (len(refs) - 1) // 2
    sources, targets, sem = refs[:count], refs[count:-1], refs[-1]
    copies = [
        pltpu.make_async_copy(source.at[0], target, sem.at[n])
        for n, (source, target) in enumerate(zip(sources, targets))
    ]
    for copy in copies:
        copy.start()
    for copy in copies:
        copy.wait()


def load(after, weights):
    hbm = pl.BlockSpec(memory_space=pltpu.HBM)
    vmem = pl.BlockSpec(memory_space=pltpu.VMEM)
    weights = [pltpu.with_memory_space_constraint(w, pltpu.HBM) for w in weights]
    return pl.pallas_call(
        load_kernel,
        in_specs=[hbm] * (1 + len(weights)),
        out_specs=(vmem,) * len(weights),
        out_shape=tuple(pltpu.VMEM(w.shape[1:], BF16) for w in weights),
        scratch_shapes=[pltpu.SemaphoreType.DMA((len(weights),))],
        compiler_params=params(1),
        cost_estimate=pl.CostEstimate(flops=10 ** 10, bytes_accessed=12 * weights[0].size, transcendentals=0),
        name="load",
    )(after, *weights)


def expert_kernel(*refs, pieces, block, out_block):
    x_refs, weight_refs, refs = refs[:pieces], refs[pieces:pieces + 6], refs[pieces + 6:]
    gate_refs, up_refs, down_refs = weight_refs[0:2], weight_refs[2:4], weight_refs[4:6]
    y_refs, (x_ref, inner_ref) = refs[:pieces], refs[pieces:]
    width, hidden = gate_refs[0].shape
    count = x_refs[0].shape[0]
    for n, ref in enumerate(x_refs):
        x_ref[n * count:(n + 1) * count, :] = ref[...]

    for half in range(2):

        def rise(i, carry, half=half):
            at = pl.ds(pl.multiple_of(i * block, block), block)
            x = x_ref[...]
            gate = dot(x, gate_refs[half][:, at])
            up = dot(x, up_refs[half][:, at])
            inner_ref[half, :, at] = (gate / (1.0 + jnp.exp(-gate)) * up).astype(BF16)
            return carry

        lax.fori_loop(0, hidden // block, rise, 0)

    def fall(i, carry):
        at = pl.ds(pl.multiple_of(i * out_block, out_block), out_block)
        total = None
        for half in range(2):
            part = dot(inner_ref[half], down_refs[half][:, at]).astype(BF16).astype(F32)
            total = part if total is None else total + part
        total = total.astype(BF16)
        for n, ref in enumerate(y_refs):
            ref[:, at] = total[n * count:(n + 1) * count, :]
        return carry

    lax.fori_loop(0, width // out_block, fall, 0)


def expert(pieces, weights):
    count, width = pieces[0].shape
    rows = count * len(pieces)
    hidden = weights[0].shape[1]
    vmem = pl.BlockSpec(memory_space=pltpu.VMEM)
    weights = [pltpu.with_memory_space_constraint(w, pltpu.VMEM) for w in weights]
    return pl.pallas_call(
        functools.partial(
            expert_kernel,
            pieces=len(pieces),
            block=256 if hidden % 256 == 0 else 128,
            out_block=512 if width % 512 == 0 else 128,
        ),
        in_specs=[vmem] * (len(pieces) + len(weights)),
        out_specs=(vmem,) * len(pieces),
        out_shape=(jax.ShapeDtypeStruct((count, width), BF16),) * len(pieces),
        scratch_shapes=[pltpu.VMEM((rows, width), BF16), pltpu.VMEM((2, rows, hidden), BF16)],
        compiler_params=params(8),
        cost_estimate=pl.CostEstimate(
            flops=12 * rows * width * hidden, bytes_accessed=8 * rows * width, transcendentals=2 * rows * hidden
        ),
        name="expert",
    )(*pieces, *weights)


def gather_kernel(*refs, pieces):
    back_refs, (pick_ref, weight_ref, own_ref, other_ref, back_ref) = refs[:pieces], refs[pieces:]
    count, rows = back_refs[0].shape[0], own_ref.shape[0]
    for n, ref in enumerate(back_refs):
        back_ref[n * count:(n + 1) * count, :] = ref[...]
    combined = None
    for k in range(pick_ref.shape[0]):
        part = dot(pick_ref[k], back_ref[...]) * weight_ref[:, k:k + 1]
        combined = part if combined is None else combined + part
    own_ref[...] = combined[:rows]
    other_ref[...] = combined[rows:].astype(BF16)


def gather(back, pick, weight):
    rows, width = weight.shape[0] // 2, back[0].shape[1]
    vmem = pl.BlockSpec(memory_space=pltpu.VMEM)
    return pl.pallas_call(
        functools.partial(gather_kernel, pieces=len(back)),
        in_specs=[vmem] * (len(back) + 2),
        out_specs=(vmem, vmem),
        out_shape=(jax.ShapeDtypeStruct((rows, width), F32), jax.ShapeDtypeStruct((rows, width), BF16)),
        scratch_shapes=[pltpu.VMEM((pick.shape[2], width), BF16)],
        compiler_params=params(20),
        name="gather",
    )(*back, pick, weight)


def finish_kernel(own_ref, other_ref, hidden_ref, gain_ref, out_ref):
    combined = own_ref[...] + other_ref[...].astype(F32)
    out_ref[...] = (hidden_ref[...].astype(F32) + rms(combined, gain_ref[...])).astype(BF16)


def finish(own, other, hidden, gain):
    return pl.pallas_call(
        finish_kernel,
        out_shape=jax.ShapeDtypeStruct(own.shape, BF16),
        compiler_params=params(16),
        name="finish",
    )(own, other, hidden, gain[None, :])


def combine_kernel(back_ref, pick_ref, weight_ref, hidden_ref, gain_ref, out_ref):
    combined = None
    for k in range(pick_ref.shape[0]):
        part = dot(pick_ref[k], back_ref[...]) * weight_ref[:, k:k + 1]
        combined = part if combined is None else combined + part
    out_ref[...] = (hidden_ref[...].astype(F32) + rms(combined, gain_ref[...])).astype(BF16)


def combine(back, pick, weight, hidden, gain):
    return pl.pallas_call(
        combine_kernel,
        out_shape=jax.ShapeDtypeStruct(hidden.shape, BF16),
        compiler_params=params(16),
        name="combine",
    )(back, pick, weight, hidden, gain[None, :])


def swap_tp(x):
    count = lax.axis_size("tp")
    return lax.ppermute(x, "tp", [(i, (i + 1) % count) for i in range(count)])


def move(x, perm):
    return lax.ppermute(x, "sp", perm)


def per_device(
    queries,
    keys,
    values,
    q_gain,
    k_gain,
    resid,
    out_weight,
    post_gain,
    ffn_gain,
    post_ffn_gain,
    gate_w,
    up_w,
    down_w,
    route_ids,
    route_w,
):
    tok_local = queries.shape[0]
    width = resid.shape[1]
    tp_count = lax.axis_size("tp")
    sp_count = lax.axis_size("sp")
    top_count = route_ids.shape[1]
    expert_count = gate_w.shape[0] * sp_count
    capacity = 3 * tok_local * top_count // (2 * tp_count * expert_count)
    slots = expert_count * capacity

    tp_index = lax.axis_index("tp").astype(jnp.int32).reshape(1)
    sp_index = lax.axis_index("sp").astype(jnp.int32).reshape(1)
    paired = tp_count == 2 and expert_count == sp_count == 16 and capacity % 8 == 0

    qn, kv = prep(queries, keys, values, q_gain, k_gain)

    far = 4
    plane = sp_count // far
    over_z = lambda x, d: move(x, [(i, (i // plane ^ d) * plane + i % plane) for i in range(sp_count)])
    in_plane = lambda x: [move(x, [(i, i ^ d) for i in range(sp_count)]) for d in range(1, plane)]
    z_blocks = [over_z(kv, d) for d in range(1, far)]
    early = [kv, z_blocks[0]] + in_plane(kv) + in_plane(z_blocks[0])
    late = z_blocks[1:] + in_plane(jnp.concatenate(z_blocks[1:], axis=0))

    ids, shares, resids = [route_ids.T], [route_w.T], [resid]
    _, out_w, ids, shares, resids = lax.optimization_barrier((kv, out_weight, ids, shares, resids))
    if paired:
        ids.append(swap_tp(ids[0]))
        shares.append(swap_tp(shares[0]))
        resids.append(swap_tp(resids[0]))
    w_other = swap_tp(out_w)
    gate_w, up_w, down_w, _ = lax.optimization_barrier((gate_w, up_w, down_w, z_blocks[0]))
    gates = (gate_w, swap_tp(gate_w))
    ups = (up_w, swap_tp(up_w))
    downs = (down_w, swap_tp(down_w))
    pick, weight, pack = route(ids + shares, jnp.concatenate([sp_index, tp_index]), expert_count, capacity)

    carry = attend(qn, early, None, False)
    attended = attend(qn, late, carry, True)
    hidden, *outgoing = project(
        tp_index,
        attended,
        swap_tp(attended),
        out_weight,
        w_other,
        resids,
        post_gain,
        ffn_gain,
        pack,
        sp_count // 2 if paired else 1,
    )
    weights = load(hidden, gates + ups + downs)
    if not paired:
        swap_all = lambda x: lax.all_to_all(
            x.reshape(expert_count, capacity, width), "sp", split_axis=0, concat_axis=0, tiled=True
        ).reshape(slots, width)
        returned = swap_all(expert([swap_all(outgoing[0])], weights)[0])
        return combine(returned, pick, weight, hidden, post_ffn_gain)

    def move_pair(x, j):
        perm = [(2 * i + t, 2 * (i ^ (2 * j + t)) + t) for i in range(sp_count) for t in range(2)]
        return lax.ppermute(x, ("sp", "tp"), perm)

    stages = ((6, 5, 3, 0), (7, 4, 2, 1))
    arrived = [[move_pair(outgoing[j], j) for j in stage] for stage in stages]
    returned = [None] * len(outgoing)
    done = None
    for stage, pieces in zip(stages, arrived):
        if done is not None:
            pieces, _ = lax.optimization_barrier((pieces, done))
        done = expert(pieces, weights)
        for j, piece in zip(stage, done):
            returned[j] = move_pair(piece, j)
    combined, for_other = gather(returned, pick, weight)
    return finish(combined, swap_tp(for_other), hidden, post_ffn_gain)


def solution(mesh):
    in_specs = (
        P("sp", "tp"),
        P("sp", "tp"),
        P("sp", "tp"),
        P(),
        P(),
        P(("sp", "tp"), None),
        P("tp", None),
        P(),
        P(),
        P(),
        P("sp", None, "tp"),
        P("sp", None, "tp"),
        P("sp", "tp", None),
        P(("sp", "tp"), None),
        P(("sp", "tp"), None),
    )
    out_specs = P(("sp", "tp"), None)
    return jax.shard_map(
        per_device, mesh=mesh, in_specs=in_specs, out_specs=out_specs, check_vma=False
    )
```

```python
import functools

import jax
import jax.numpy as jnp
import numpy as np
from jax import lax
from jax.experimental import pallas as pl
from jax.experimental.pallas import tpu as pltpu
from jax.sharding import PartitionSpec as P


HEAD_DIM = 64
GRID_W = 64
LANES = 128
EPS = 1e-06
THETA = 10000.0
MIB = 1024 * 1024
F32 = jnp.float32
BF16 = jnp.bfloat16


def dot(a, b):
    return jnp.dot(a, b, preferred_element_type=F32)


def dot_t(a, b):
    return lax.dot_general(a, b, (((1,), (1,)), ((), ())), preferred_element_type=F32)


def params(mib):
    return pltpu.CompilerParams(vmem_limit_bytes=mib * MIB)


def prep_kernel(base_ref, q_ref, k_ref, v_ref, freq_ref, qg_ref, kg_ref, qn_ref, kv_ref):
    tok = q_ref.shape[0]
    grid_rows = tok // GRID_W
    row = lax.broadcasted_iota(jnp.int32, (LANES, LANES), 0)
    col = lax.broadcasted_iota(jnp.int32, (LANES, LANES), 1)
    swap = jnp.where(row == (col ^ 1), 1.0, 0.0).astype(BF16)
    mean = jnp.where((row // HEAD_DIM) == (col // HEAD_DIM), 1.0 / HEAD_DIM, 0.0).astype(BF16)
    lane = lax.broadcasted_iota(jnp.int32, (tok, LANES), 1)

    def angles(first, count):
        place = first + lax.broadcasted_iota(jnp.int32, (count, LANES), 0)
        return place.astype(F32) * freq_ref[...]

    sign = jnp.where(lax.broadcasted_iota(jnp.int32, (1, LANES), 1) % 2 == 0, -1.0, 1.0)
    by_row = angles(base_ref[0] // GRID_W, max(8, grid_rows))
    by_col = angles(0, GRID_W)
    row_lanes = lax.broadcasted_iota(jnp.int32, (GRID_W, LANES), 1) % HEAD_DIM < HEAD_DIM // 2

    def spread(rows, cols):
        parts = [
            jnp.where(row_lanes, jnp.broadcast_to(rows[i:i + 1], (GRID_W, LANES)), cols) for i in range(grid_rows)
        ]
        return jnp.concatenate(parts, axis=0)

    cos = spread(jnp.cos(by_row), jnp.cos(by_col))
    sin = spread(jnp.sin(by_row) * sign, jnp.sin(by_col) * sign)

    def factors(gain_ref):
        gain = jnp.broadcast_to(jnp.concatenate([gain_ref[...]] * 2, axis=1), (8, LANES))
        even = lax.broadcasted_iota(jnp.int32, (8, LANES), 1) % 2 == 0
        swapped = jnp.where(even, pltpu.roll(gain, LANES - 1, 1), pltpu.roll(gain, 1, 1))
        return cos * gain[:1], sin * swapped[:1]

    def turn(x, cos_gain, sin_gain):
        x32 = x.astype(F32)
        square = x32 * x32
        high = square.astype(BF16)
        low = (square - high.astype(F32)).astype(BF16)
        scale = lax.rsqrt(dot(high, mean) + dot(low, mean) + EPS)
        return (x32 * cos_gain + dot(x, swap) * sin_gain) * scale

    kv_ref[:, :LANES] = turn(k_ref[...], *factors(kg_ref)).astype(BF16)
    kv_ref[:, LANES:] = v_ref[...]
    heads = q_ref.shape[1] // HEAD_DIM
    group = heads // 2
    q_factors = factors(qg_ref)
    for pair in range(heads // 2):
        out = turn(q_ref[:, pair * LANES:(pair + 1) * LANES], *q_factors) * (HEAD_DIM ** -0.5)
        rolled = pltpu.roll(out, HEAD_DIM, 1)
        for side in range(2):
            head = 2 * pair + side
            kv = head // group
            source = out if side == kv else rolled
            qn_ref[head] = jnp.where((lane // HEAD_DIM) == kv, source, 0.0).astype(BF16)


def prep(queries, keys, values, q_gain, k_gain):
    tok = queries.shape[0]
    heads = queries.shape[1] // HEAD_DIM
    base = (lax.axis_index("sp") * tok).astype(jnp.int32).reshape(1)
    half = HEAD_DIM // 2
    freqs = (THETA ** (-((np.arange(LANES) % half) // 2 * 2) / half)).astype(np.float32)[None, :]
    vmem = pl.BlockSpec(memory_space=pltpu.VMEM)
    return pl.pallas_call(
        prep_kernel,
        in_specs=[pl.BlockSpec(memory_space=pltpu.SMEM)] + [vmem] * 6,
        out_specs=(vmem, vmem),
        out_shape=(
            pltpu.VMEM((heads, tok, LANES), BF16),
            pltpu.VMEM((tok, 2 * LANES), BF16),
        ),
        compiler_params=params(56),
        name="prep",
    )(base, queries, keys, values, jnp.asarray(freqs), q_gain[None, :], k_gain[None, :])


def route_kernel(place_ref, *refs, sources, top, experts, capacity):
    meta_refs, (pick_ref, weight_ref, pack_ref) = refs[:2 * sources], refs[2 * sources:]
    block = meta_refs[0].shape[1]
    rows, slots = sources * block, pack_ref.shape[0]
    flat = jnp.concatenate([ref[...].astype(F32) for ref in meta_refs], axis=0)
    flat = jnp.concatenate([flat] * (8 // flat.shape[0]), axis=0).T
    stack = lambda first: [
        jnp.concatenate([flat[:, first + s * top + k:first + s * top + k + 1] for s in range(sources)], axis=0)
        for k in range(top)
    ]
    ids = [column.astype(jnp.int32) for column in stack(0)]
    weight_ref[...] = jnp.concatenate(stack(sources * top), axis=1)
    lane = lax.broadcasted_iota(jnp.int32, (rows, experts), 1)
    chosen = [jnp.where(e == lane, 1.0, 0.0) for e in ids]
    both = chosen[0]
    for c in chosen[1:]:
        both = both + c
    row = lax.broadcasted_iota(jnp.int32, (rows, rows), 0)
    col = lax.broadcasted_iota(jnp.int32, (rows, rows), 1)
    before = (col < row) & (col // block == row // block)
    earlier = dot(jnp.where(before, 1.0, 0.0).astype(BF16), both.astype(BF16))
    number = lax.broadcasted_iota(jnp.int32, (rows, slots), 1)
    source = lax.broadcasted_iota(jnp.int32, (rows, 1), 0) // block
    packed = None
    for k in range(top):
        rank = jnp.sum(earlier * chosen[k], axis=1, keepdims=True).astype(jnp.int32)
        if sources == 2:
            mask = ids[k] ^ place_ref[0]
            slot = ((mask // 2) * 2 + source) * capacity + rank
            slot = jnp.where(mask % 2 == place_ref[1], slot, -1)
        else:
            slot = ids[k] * capacity + rank
        pick = jnp.where(number == slot, 1.0, 0.0)
        pick_ref[k] = pick.astype(BF16)
        packed = pick if packed is None else packed + pick
    unit = jnp.where(row == col, 1.0, 0.0).astype(BF16)
    pack_ref[...] = lax.dot_general(
        packed.astype(BF16), unit, (((0,), (0,)), ((), ())), preferred_element_type=F32
    ).astype(BF16)


def route(metas, place, experts, capacity):
    top, block = metas[0].shape
    sources = len(metas) // 2
    rows, slots = sources * block, experts * capacity
    vmem = pl.BlockSpec(memory_space=pltpu.VMEM)
    return pl.pallas_call(
        functools.partial(route_kernel, sources=sources, top=top, experts=experts, capacity=capacity),
        in_specs=[pl.BlockSpec(memory_space=pltpu.SMEM)] + [vmem] * len(metas),
        out_specs=(vmem,) * 3,
        out_shape=(
            jax.ShapeDtypeStruct((top, rows, slots), BF16),
            jax.ShapeDtypeStruct((rows, top), F32),
            jax.ShapeDtypeStruct((slots, rows), BF16),
        ),
        compiler_params=params(16),
        name="route",
    )(place, *metas)


def attend_kernel(*refs, counts, first, last, heads_step):
    q_ref = refs[0]
    n = len(counts)
    kv_refs = refs[1:1 + n]
    at = 1 + n
    if not first:
        m_in, acc_in = refs[at:at + 2]
        at += 2
    if last:
        out_ref = refs[at]
        at += 1
    else:
        m_out, acc_out = refs[at:at + 2]
        at += 2
    vaug = refs[at]
    tok = q_ref.shape[1]
    step = pl.program_id(0)

    blocks = []
    for ref, count in zip(kv_refs, counts):
        for c in range(count):
            blocks.append((ref, c * tok))

    @pl.when(step == 0)
    def _():
        for b, (ref, at_row) in enumerate(blocks):
            vaug[b * tok:(b + 1) * tok, :LANES] = ref[at_row:at_row + tok, LANES:]
            vaug[b * tok:(b + 1) * tok, LANES:] = jnp.ones((tok, LANES), BF16)

    outs = []
    for h in range(heads_step):
        q = q_ref[h]
        scores = [dot_t(q, ref[at_row:at_row + tok, :LANES]) for ref, at_row in blocks]
        top = scores[0]
        for s in scores[1:]:
            top = jnp.maximum(top, s)
        m = jnp.max(top, axis=1, keepdims=True)
        if not first:
            before = m_in[h][:, :1]
            m = jnp.maximum(m, before)
        weights = jnp.concatenate([jnp.exp(s - m).astype(BF16) for s in scores], axis=1)
        acc = dot(weights, vaug[...])
        if not first:
            acc = acc + acc_in[h] * jnp.exp(before - m)
        if last:
            outs.append(acc[:, :LANES] / acc[:, LANES:])
        else:
            m_out[h] = jnp.broadcast_to(m, (tok, LANES))
            acc_out[h] = acc
    if last:
        lane = lax.broadcasted_iota(jnp.int32, (tok, LANES), 1)
        group_steps = pl.num_programs(0) // 2
        kv = step // group_steps
        for pair in range(heads_step // 2):
            a, b = outs[2 * pair], outs[2 * pair + 1]
            low = jnp.where(lane < HEAD_DIM, a, pltpu.roll(b, HEAD_DIM, 1))
            high = jnp.where(lane < HEAD_DIM, pltpu.roll(a, HEAD_DIM, 1), b)
            out_ref[:, pair * LANES:(pair + 1) * LANES] = jnp.where(kv == 0, low, high).astype(BF16)


def attend(qn, kv_list, carry, last, heads_step=4):
    heads, tok, _ = qn.shape
    counts = tuple(kv.shape[0] // tok for kv in kv_list)
    first = carry is None
    whole = lambda shape: pl.BlockSpec(shape, lambda i: (0,) * len(shape))
    head_spec = lambda width: pl.BlockSpec((heads_step, tok, width), lambda i: (i, 0, 0))
    in_specs = [head_spec(LANES)] + [whole(kv.shape) for kv in kv_list]
    args = [qn, *kv_list]
    if not first:
        in_specs += [head_spec(LANES), head_spec(2 * LANES)]
        args += list(carry)
    if last:
        out_shape = jax.ShapeDtypeStruct((tok, heads * HEAD_DIM), BF16)
        out_specs = pl.BlockSpec((tok, heads_step * HEAD_DIM), lambda i: (0, i))
    else:
        out_shape = (
            jax.ShapeDtypeStruct((heads, tok, LANES), F32),
            jax.ShapeDtypeStruct((heads, tok, 2 * LANES), F32),
        )
        out_specs = (head_spec(LANES), head_spec(2 * LANES))
    total = sum(counts) * tok
    return pl.pallas_call(
        functools.partial(attend_kernel, counts=counts, first=first, last=last, heads_step=heads_step),
        grid=(heads // heads_step,),
        in_specs=in_specs,
        out_specs=out_specs,
        out_shape=out_shape,
        scratch_shapes=[pltpu.VMEM((total, 2 * LANES), BF16)],
        compiler_params=params(28),
        cost_estimate=pl.CostEstimate(
            flops=4 * heads * tok * total * 256, bytes_accessed=total * 512, transcendentals=heads * tok * total
        ),
        name="attend",
    )(*args)


def rms(x, gain):
    return x * lax.rsqrt(jnp.mean(x * x, axis=-1, keepdims=True) + EPS) * gain


def project_kernel(tp_ref, own_ref, other_ref, w_own, w_other, *refs, sources):
    resid_refs, refs = refs[:sources], refs[sources:]
    pg_ref, fg_ref, pack_ref, hidden_ref, *out_refs = refs
    rows = hidden_ref.shape[0]
    order = (tp_ref[0], 1 - tp_ref[0])[:sources]

    normed = []
    for n, t in enumerate(order):
        span = pl.ds(pl.multiple_of(t * rows, rows), rows)
        mixed = dot(own_ref[span, :], w_own[...]) + dot(other_ref[span, :], w_other[...])
        hidden = (resid_refs[n][...].astype(F32) + rms(mixed, pg_ref[...])).astype(BF16)
        if n == 0:
            hidden_ref[...] = hidden
        normed.append(rms(hidden.astype(F32), fg_ref[...]).astype(BF16))
    normed = jnp.concatenate(normed, axis=0)
    count = out_refs[0].shape[0]
    for n, ref in enumerate(out_refs):
        ref[...] = dot(pack_ref[n * count:(n + 1) * count, :], normed).astype(BF16)


def project(tp_index, own, other, w_own, w_other, resids, post_gain, ffn_gain, pack, pieces):
    rows, width = resids[0].shape
    count = pack.shape[0] // pieces
    vmem = pl.BlockSpec(memory_space=pltpu.VMEM)
    return pl.pallas_call(
        functools.partial(project_kernel, sources=len(resids)),
        in_specs=[pl.BlockSpec(memory_space=pltpu.SMEM)] + [vmem] * (7 + len(resids)),
        out_specs=(vmem,) * (1 + pieces),
        out_shape=(jax.ShapeDtypeStruct((rows, width), BF16),)
        + (jax.ShapeDtypeStruct((count, width), BF16),) * pieces,
        compiler_params=params(24),
        name="project",
    )(tp_index, own, other, w_own, w_other, *resids, post_gain[None, :], ffn_gain[None, :], pack)


def load_kernel(after_ref, *refs):
    count = (len(refs) - 1) // 2
    sources, targets, sem = refs[:count], refs[count:-1], refs[-1]
    copies = [
        pltpu.make_async_copy(source.at[0], target, sem.at[n])
        for n, (source, target) in enumerate(zip(sources, targets))
    ]
    for copy in copies:
        copy.start()
    for copy in copies:
        copy.wait()


def load(after, weights):
    hbm = pl.BlockSpec(memory_space=pltpu.HBM)
    vmem = pl.BlockSpec(memory_space=pltpu.VMEM)
    weights = [pltpu.with_memory_space_constraint(w, pltpu.HBM) for w in weights]
    return pl.pallas_call(
        load_kernel,
        in_specs=[hbm] * (1 + len(weights)),
        out_specs=(vmem,) * len(weights),
        out_shape=tuple(pltpu.VMEM(w.shape[1:], BF16) for w in weights),
        scratch_shapes=[pltpu.SemaphoreType.DMA((len(weights),))],
        compiler_params=params(1),
        cost_estimate=pl.CostEstimate(flops=10 ** 10, bytes_accessed=12 * weights[0].size, transcendentals=0),
        name="load",
    )(after, *weights)


def expert_kernel(*refs, pieces, block, out_block, fetch):
    x_refs, refs = refs[:pieces], refs[pieces:]
    gate_refs, up_refs, down_refs, refs = refs[0:2], refs[2:4], refs[4:6], refs[6:]
    y_refs, refs = refs[:pieces], refs[pieces:]
    copies = ()
    if fetch:
        down_hbm, down_refs, sem, refs = down_refs, refs[:2], refs[-1], refs[2:-1]
        copies = [pltpu.make_async_copy(down_hbm[n].at[0], down_refs[n], sem.at[n]) for n in range(2)]
    for copy in copies:
        copy.start()
    x_ref, inner_ref = refs
    width, hidden = gate_refs[0].shape
    count = x_refs[0].shape[0]
    for n, ref in enumerate(x_refs):
        x_ref[n * count:(n + 1) * count, :] = ref[...]

    for half in range(2):

        def rise(i, carry, half=half):
            at = pl.ds(pl.multiple_of(i * block, block), block)
            x = x_ref[...]
            gate = dot(x, gate_refs[half][:, at])
            up = dot(x, up_refs[half][:, at])
            inner_ref[half, :, at] = (gate / (1.0 + jnp.exp(-gate)) * up).astype(BF16)
            return carry

        lax.fori_loop(0, hidden // block, rise, 0)

    for copy in copies:
        copy.wait()

    def fall(i, carry):
        at = pl.ds(pl.multiple_of(i * out_block, out_block), out_block)
        total = None
        for half in range(2):
            part = dot(inner_ref[half], down_refs[half][:, at]).astype(BF16).astype(F32)
            total = part if total is None else total + part
        total = total.astype(BF16)
        for n, ref in enumerate(y_refs):
            ref[:, at] = total[n * count:(n + 1) * count, :]
        return carry

    lax.fori_loop(0, width // out_block, fall, 0)


def expert(pieces, rises, falls, fetch):
    count, width = pieces[0].shape
    rows = count * len(pieces)
    hidden = rises[0].shape[1]
    vmem = pl.BlockSpec(memory_space=pltpu.VMEM)
    hbm = pl.BlockSpec(memory_space=pltpu.HBM)
    rises = [pltpu.with_memory_space_constraint(w, pltpu.VMEM) for w in rises]
    falls = [pltpu.with_memory_space_constraint(w, pltpu.HBM if fetch else pltpu.VMEM) for w in falls]
    kept = tuple(pltpu.VMEM((hidden, width), BF16) for _ in falls) if fetch else ()
    out = pl.pallas_call(
        functools.partial(
            expert_kernel,
            pieces=len(pieces),
            block=256 if hidden % 256 == 0 else 128,
            out_block=512 if width % 512 == 0 else 128,
            fetch=fetch,
        ),
        in_specs=[vmem] * (len(pieces) + len(rises)) + [hbm if fetch else vmem] * 2,
        out_specs=(vmem,) * (len(pieces) + len(kept)),
        out_shape=(jax.ShapeDtypeStruct((count, width), BF16),) * len(pieces) + kept,
        scratch_shapes=[pltpu.VMEM((rows, width), BF16), pltpu.VMEM((2, rows, hidden), BF16)]
        + ([pltpu.SemaphoreType.DMA((2,))] if fetch else []),
        compiler_params=params(max(8, rows // 24)),
        cost_estimate=pl.CostEstimate(
            flops=12 * rows * width * hidden, bytes_accessed=8 * rows * width, transcendentals=2 * rows * hidden
        ),
        name="expert",
    )(*pieces, *rises, *falls)
    return out[:len(pieces)], out[len(pieces):]


def gather_kernel(*refs, pieces):
    back_refs, (pick_ref, weight_ref, own_ref, other_ref, back_ref) = refs[:pieces], refs[pieces:]
    count, rows = back_refs[0].shape[0], own_ref.shape[0]
    for n, ref in enumerate(back_refs):
        back_ref[n * count:(n + 1) * count, :] = ref[...]
    combined = None
    for k in range(pick_ref.shape[0]):
        part = dot(pick_ref[k], back_ref[...]) * weight_ref[:, k:k + 1]
        combined = part if combined is None else combined + part
    own_ref[...] = combined[:rows]
    other_ref[...] = combined[rows:].astype(BF16)


def gather(back, pick, weight):
    rows, width = weight.shape[0] // 2, back[0].shape[1]
    vmem = pl.BlockSpec(memory_space=pltpu.VMEM)
    return pl.pallas_call(
        functools.partial(gather_kernel, pieces=len(back)),
        in_specs=[vmem] * (len(back) + 2),
        out_specs=(vmem, vmem),
        out_shape=(jax.ShapeDtypeStruct((rows, width), F32), jax.ShapeDtypeStruct((rows, width), BF16)),
        scratch_shapes=[pltpu.VMEM((pick.shape[2], width), BF16)],
        compiler_params=params(20),
        name="gather",
    )(*back, pick, weight)


def finish_kernel(own_ref, other_ref, hidden_ref, gain_ref, out_ref):
    combined = own_ref[...] + other_ref[...].astype(F32)
    out_ref[...] = (hidden_ref[...].astype(F32) + rms(combined, gain_ref[...])).astype(BF16)


def finish(own, other, hidden, gain):
    return pl.pallas_call(
        finish_kernel,
        out_shape=jax.ShapeDtypeStruct(own.shape, BF16),
        compiler_params=params(16),
        name="finish",
    )(own, other, hidden, gain[None, :])


def combine_kernel(back_ref, pick_ref, weight_ref, hidden_ref, gain_ref, out_ref):
    combined = None
    for k in range(pick_ref.shape[0]):
        part = dot(pick_ref[k], back_ref[...]) * weight_ref[:, k:k + 1]
        combined = part if combined is None else combined + part
    out_ref[...] = (hidden_ref[...].astype(F32) + rms(combined, gain_ref[...])).astype(BF16)


def combine(back, pick, weight, hidden, gain):
    return pl.pallas_call(
        combine_kernel,
        out_shape=jax.ShapeDtypeStruct(hidden.shape, BF16),
        compiler_params=params(16),
        name="combine",
    )(back, pick, weight, hidden, gain[None, :])


def swap_tp(x):
    count = lax.axis_size("tp")
    return lax.ppermute(x, "tp", [(i, (i + 1) % count) for i in range(count)])


def move(x, perm):
    return lax.ppermute(x, "sp", perm)


def per_device(
    queries,
    keys,
    values,
    q_gain,
    k_gain,
    resid,
    out_weight,
    post_gain,
    ffn_gain,
    post_ffn_gain,
    gate_w,
    up_w,
    down_w,
    route_ids,
    route_w,
):
    tok_local = queries.shape[0]
    width = resid.shape[1]
    tp_count = lax.axis_size("tp")
    sp_count = lax.axis_size("sp")
    top_count = route_ids.shape[1]
    expert_count = gate_w.shape[0] * sp_count
    capacity = 3 * tok_local * top_count // (2 * tp_count * expert_count)
    slots = expert_count * capacity

    tp_index = lax.axis_index("tp").astype(jnp.int32).reshape(1)
    sp_index = lax.axis_index("sp").astype(jnp.int32).reshape(1)
    paired = tp_count == 2 and expert_count == sp_count == 16 and capacity % 8 == 0

    qn, kv = prep(queries, keys, values, q_gain, k_gain)

    far = 4
    plane = sp_count // far

    def over_z(d):
        return move(kv, [(i, (i // plane ^ d) * plane + i % plane) for i in range(sp_count)])

    def in_plane(x):
        out = []
        for d in range(1, plane):
            out.append(move(x, [(i, i ^ d) for i in range(sp_count)]))
        return out

    z_blocks = [over_z(d) for d in range(1, far)]
    early = [kv, z_blocks[0]] + in_plane(kv) + in_plane(z_blocks[0])
    late = z_blocks[1:] + in_plane(jnp.concatenate(z_blocks[1:], axis=0))

    ids, shares, resids = [route_ids.T], [route_w.T], [resid]
    if paired:
        ids.append(swap_tp(ids[0]))
        shares.append(swap_tp(shares[0]))
        resids.append(swap_tp(resid))
    w_other = swap_tp(out_weight)
    gates = (gate_w, swap_tp(gate_w))
    ups = (up_w, swap_tp(up_w))
    downs = (down_w, swap_tp(down_w))
    pick, weight, pack = route(ids + shares, jnp.concatenate([sp_index, tp_index]), expert_count, capacity)

    carry = attend(qn, early, None, False)
    attended = attend(qn, late, carry, True)
    hidden, *outgoing = project(
        tp_index,
        attended,
        swap_tp(attended),
        out_weight,
        w_other,
        resids,
        post_gain,
        ffn_gain,
        pack,
        sp_count // 2 if paired else 1,
    )
    loaded = load(hidden, gates + ups + (() if paired else downs))
    if not paired:
        swap_all = lambda x: lax.all_to_all(
            x.reshape(expert_count, capacity, width), "sp", split_axis=0, concat_axis=0, tiled=True
        ).reshape(slots, width)
        returned = swap_all(expert([swap_all(outgoing[0])], loaded[:4], loaded[4:], False)[0][0])
        return combine(returned, pick, weight, hidden, post_ffn_gain)

    def move_pair(x, j):
        perm = [(2 * i + t, 2 * (i ^ (2 * j + t)) + t) for i in range(sp_count) for t in range(2)]
        return lax.ppermute(x, ("sp", "tp"), perm)

    stages = ((6, 5, 3, 0), (7, 4, 2, 1))
    arrived = []
    for n, stage in enumerate(stages):
        arrived.append([])
        for j in stage:
            arrived[n].append(move_pair(outgoing[j], j))
    returned = [None] * len(outgoing)
    done = None
    for n, (stage, pieces) in enumerate(zip(stages, arrived)):
        if done is not None:
            pieces, _ = lax.optimization_barrier((pieces, done))
        done, kept = expert(pieces, loaded, downs, n == 0)
        downs = kept or downs
        for j, piece in zip(stage, done):
            returned[j] = move_pair(piece, j)
    combined, for_other = gather(returned, pick, weight)
    return finish(combined, swap_tp(for_other), hidden, post_ffn_gain)


def solution(mesh):
    in_specs = (
        P("sp", "tp"),
        P("sp", "tp"),
        P("sp", "tp"),
        P(),
        P(),
        P(("sp", "tp"), None),
        P("tp", None),
        P(),
        P(),
        P(),
        P("sp", None, "tp"),
        P("sp", None, "tp"),
        P("sp", "tp", None),
        P(("sp", "tp"), None),
        P(("sp", "tp"), None),
    )
    out_specs = P(("sp", "tp"), None)
    return jax.shard_map(
        per_device, mesh=mesh, in_specs=in_specs, out_specs=out_specs, check_vma=False
    )
```

```python
import functools

import jax
import jax.numpy as jnp
import numpy as np
from jax import lax
from jax.experimental import pallas as pl
from jax.experimental.pallas import tpu as pltpu
from jax.sharding import PartitionSpec as P


HEAD_DIM = 64
GRID_W = 64
LANES = 128
EPS = 1e-06
THETA = 10000.0
MIB = 1024 * 1024
F32 = jnp.float32
BF16 = jnp.bfloat16


def dot(a, b):
    return jnp.dot(a, b, preferred_element_type=F32)


def dot_t(a, b):
    return lax.dot_general(a, b, (((1,), (1,)), ((), ())), preferred_element_type=F32)


def params(mib):
    return pltpu.CompilerParams(vmem_limit_bytes=mib * MIB)


def prep_kernel(base_ref, q_ref, k_ref, v_ref, freq_ref, qg_ref, kg_ref, qn_ref, kv_ref):
    tok = q_ref.shape[0]
    grid_rows = tok // GRID_W
    row = lax.broadcasted_iota(jnp.int32, (LANES, LANES), 0)
    col = lax.broadcasted_iota(jnp.int32, (LANES, LANES), 1)
    swap = jnp.where(row == (col ^ 1), 1.0, 0.0).astype(BF16)
    mean = jnp.where((row // HEAD_DIM) == (col // HEAD_DIM), 1.0 / HEAD_DIM, 0.0).astype(BF16)
    lane = lax.broadcasted_iota(jnp.int32, (tok, LANES), 1)

    def angles(first, count):
        place = first + lax.broadcasted_iota(jnp.int32, (count, LANES), 0)
        return place.astype(F32) * freq_ref[...]

    sign = jnp.where(lax.broadcasted_iota(jnp.int32, (1, LANES), 1) % 2 == 0, -1.0, 1.0)
    by_row = angles(base_ref[0] // GRID_W, max(8, grid_rows))
    by_col = angles(0, GRID_W)
    row_lanes = lax.broadcasted_iota(jnp.int32, (GRID_W, LANES), 1) % HEAD_DIM < HEAD_DIM // 2

    def spread(rows, cols):
        parts = [
            jnp.where(row_lanes, jnp.broadcast_to(rows[i:i + 1], (GRID_W, LANES)), cols) for i in range(grid_rows)
        ]
        return jnp.concatenate(parts, axis=0)

    cos = spread(jnp.cos(by_row), jnp.cos(by_col))
    sin = spread(jnp.sin(by_row) * sign, jnp.sin(by_col) * sign)

    def factors(gain_ref):
        gain = jnp.broadcast_to(jnp.concatenate([gain_ref[...]] * 2, axis=1), (8, LANES))
        even = lax.broadcasted_iota(jnp.int32, (8, LANES), 1) % 2 == 0
        swapped = jnp.where(even, pltpu.roll(gain, LANES - 1, 1), pltpu.roll(gain, 1, 1))
        return cos * gain[:1], sin * swapped[:1]

    def turn(x, cos_gain, sin_gain):
        x32 = x.astype(F32)
        square = x32 * x32
        high = square.astype(BF16)
        low = (square - high.astype(F32)).astype(BF16)
        scale = lax.rsqrt(dot(high, mean) + dot(low, mean) + EPS)
        return (x32 * cos_gain + dot(x, swap) * sin_gain) * scale

    kv_ref[:, :LANES] = turn(k_ref[...], *factors(kg_ref)).astype(BF16)
    kv_ref[:, LANES:] = v_ref[...]
    heads = q_ref.shape[1] // HEAD_DIM
    group = heads // 2
    q_factors = factors(qg_ref)
    for pair in range(heads // 2):
        out = turn(q_ref[:, pair * LANES:(pair + 1) * LANES], *q_factors) * (HEAD_DIM ** -0.5)
        rolled = pltpu.roll(out, HEAD_DIM, 1)
        for side in range(2):
            head = 2 * pair + side
            kv = head // group
            source = out if side == kv else rolled
            qn_ref[head] = jnp.where((lane // HEAD_DIM) == kv, source, 0.0).astype(BF16)


def prep(queries, keys, values, q_gain, k_gain):
    tok = queries.shape[0]
    heads = queries.shape[1] // HEAD_DIM
    base = (lax.axis_index("sp") * tok).astype(jnp.int32).reshape(1)
    half = HEAD_DIM // 2
    freqs = (THETA ** (-((np.arange(LANES) % half) // 2 * 2) / half)).astype(np.float32)[None, :]
    vmem = pl.BlockSpec(memory_space=pltpu.VMEM)
    return pl.pallas_call(
        prep_kernel,
        in_specs=[pl.BlockSpec(memory_space=pltpu.SMEM)] + [vmem] * 6,
        out_specs=(vmem, vmem),
        out_shape=(
            pltpu.VMEM((heads, tok, LANES), BF16),
            pltpu.VMEM((tok, 2 * LANES), BF16),
        ),
        compiler_params=params(56),
        name="prep",
    )(base, queries, keys, values, jnp.asarray(freqs), q_gain[None, :], k_gain[None, :])


def route_kernel(place_ref, *refs, sources, top, experts, capacity):
    meta_refs, (pick_ref, weight_ref, pack_ref) = refs[:2 * sources], refs[2 * sources:]
    block = meta_refs[0].shape[1]
    rows, slots = sources * block, pack_ref.shape[0]
    flat = jnp.concatenate([ref[...].astype(F32) for ref in meta_refs], axis=0)
    flat = jnp.concatenate([flat] * (8 // flat.shape[0]), axis=0).T
    stack = lambda first: [
        jnp.concatenate([flat[:, first + s * top + k:first + s * top + k + 1] for s in range(sources)], axis=0)
        for k in range(top)
    ]
    ids = [column.astype(jnp.int32) for column in stack(0)]
    weight_ref[...] = jnp.concatenate(stack(sources * top), axis=1)
    lane = lax.broadcasted_iota(jnp.int32, (rows, experts), 1)
    chosen = [jnp.where(e == lane, 1.0, 0.0) for e in ids]
    both = chosen[0]
    for c in chosen[1:]:
        both = both + c
    row = lax.broadcasted_iota(jnp.int32, (rows, rows), 0)
    col = lax.broadcasted_iota(jnp.int32, (rows, rows), 1)
    before = (col < row) & (col // block == row // block)
    earlier = dot(jnp.where(before, 1.0, 0.0).astype(BF16), both.astype(BF16))
    number = lax.broadcasted_iota(jnp.int32, (rows, slots), 1)
    source = lax.broadcasted_iota(jnp.int32, (rows, 1), 0) // block
    packed = None
    for k in range(top):
        rank = jnp.sum(earlier * chosen[k], axis=1, keepdims=True).astype(jnp.int32)
        if sources == 2:
            mask = ids[k] ^ place_ref[0]
            slot = ((mask // 2) * 2 + source) * capacity + rank
            slot = jnp.where(mask % 2 == place_ref[1], slot, -1)
        else:
            slot = ids[k] * capacity + rank
        pick = jnp.where(number == slot, 1.0, 0.0)
        pick_ref[k] = pick.astype(BF16)
        packed = pick if packed is None else packed + pick
    unit = jnp.where(row == col, 1.0, 0.0).astype(BF16)
    pack_ref[...] = lax.dot_general(
        packed.astype(BF16), unit, (((0,), (0,)), ((), ())), preferred_element_type=F32
    ).astype(BF16)


def route(metas, place, experts, capacity):
    top, block = metas[0].shape
    sources = len(metas) // 2
    rows, slots = sources * block, experts * capacity
    vmem = pl.BlockSpec(memory_space=pltpu.VMEM)
    return pl.pallas_call(
        functools.partial(route_kernel, sources=sources, top=top, experts=experts, capacity=capacity),
        in_specs=[pl.BlockSpec(memory_space=pltpu.SMEM)] + [vmem] * len(metas),
        out_specs=(vmem,) * 3,
        out_shape=(
            jax.ShapeDtypeStruct((top, rows, slots), BF16),
            jax.ShapeDtypeStruct((rows, top), F32),
            jax.ShapeDtypeStruct((slots, rows), BF16),
        ),
        compiler_params=params(16),
        name="route",
    )(place, *metas)


def attend_kernel(*refs, counts, first, last, heads_step):
    q_ref = refs[0]
    n = len(counts)
    kv_refs = refs[1:1 + n]
    at = 1 + n
    if not first:
        m_in, acc_in = refs[at:at + 2]
        at += 2
    if last:
        out_ref = refs[at]
        at += 1
    else:
        m_out, acc_out = refs[at:at + 2]
        at += 2
    vaug = refs[at]
    tok = q_ref.shape[1]
    step = pl.program_id(0)

    blocks = []
    for ref, count in zip(kv_refs, counts):
        for c in range(count):
            blocks.append((ref, c * tok))

    @pl.when(step == 0)
    def _():
        for b, (ref, at_row) in enumerate(blocks):
            vaug[b * tok:(b + 1) * tok, :LANES] = ref[at_row:at_row + tok, LANES:]
            vaug[b * tok:(b + 1) * tok, LANES:] = jnp.ones((tok, LANES), BF16)

    outs = []
    for h in range(heads_step):
        q = q_ref[h]
        scores = [dot_t(q, ref[at_row:at_row + tok, :LANES]) for ref, at_row in blocks]
        top = scores[0]
        for s in scores[1:]:
            top = jnp.maximum(top, s)
        m = jnp.max(top, axis=1, keepdims=True)
        if not first:
            before = m_in[h][:, :1]
            m = jnp.maximum(m, before)
        weights = jnp.concatenate([jnp.exp(s - m).astype(BF16) for s in scores], axis=1)
        acc = dot(weights, vaug[...])
        if not first:
            acc = acc + acc_in[h] * jnp.exp(before - m)
        if last:
            outs.append(acc[:, :LANES] / acc[:, LANES:])
        else:
            m_out[h] = jnp.broadcast_to(m, (tok, LANES))
            acc_out[h] = acc
    if last:
        lane = lax.broadcasted_iota(jnp.int32, (tok, LANES), 1)
        for pair in range(heads_step // 2):
            a, b = outs[2 * pair], outs[2 * pair + 1]
            kv = (2 * pair) // (heads_step // 2)
            low = jnp.where(lane < HEAD_DIM, a, pltpu.roll(b, HEAD_DIM, 1))
            high = jnp.where(lane < HEAD_DIM, pltpu.roll(a, HEAD_DIM, 1), b)
            out_ref[:, pair * LANES:(pair + 1) * LANES] = (high if kv else low).astype(BF16)


def attend(qn, kv_list, carry, last, heads_step=8):
    heads, tok, _ = qn.shape
    counts = tuple(kv.shape[0] // tok for kv in kv_list)
    first = carry is None
    whole = lambda shape: pl.BlockSpec(shape, lambda i: (0,) * len(shape))
    head_spec = lambda width: pl.BlockSpec((heads_step, tok, width), lambda i: (i, 0, 0))
    in_specs = [head_spec(LANES)] + [whole(kv.shape) for kv in kv_list]
    args = [qn, *kv_list]
    if not first:
        in_specs += [head_spec(LANES), head_spec(2 * LANES)]
        args += list(carry)
    if last:
        out_shape = jax.ShapeDtypeStruct((tok, heads * HEAD_DIM), BF16)
        out_specs = pl.BlockSpec((tok, heads_step * HEAD_DIM), lambda i: (0, i))
    else:
        out_shape = (
            jax.ShapeDtypeStruct((heads, tok, LANES), F32),
            jax.ShapeDtypeStruct((heads, tok, 2 * LANES), F32),
        )
        out_specs = (head_spec(LANES), head_spec(2 * LANES))
    total = sum(counts) * tok
    return pl.pallas_call(
        functools.partial(attend_kernel, counts=counts, first=first, last=last, heads_step=heads_step),
        grid=(heads // heads_step,),
        in_specs=in_specs,
        out_specs=out_specs,
        out_shape=out_shape,
        scratch_shapes=[pltpu.VMEM((total, 2 * LANES), BF16)],
        compiler_params=params(28),
        cost_estimate=pl.CostEstimate(
            flops=4 * heads * tok * total * 256, bytes_accessed=total * 512, transcendentals=heads * tok * total
        ),
        name="attend",
    )(*args)


def rms(x, gain):
    return x * lax.rsqrt(jnp.mean(x * x, axis=-1, keepdims=True) + EPS) * gain


def project_kernel(tp_ref, own_ref, other_ref, w_own, w_other, *refs, sources):
    resid_refs, refs = refs[:sources], refs[sources:]
    pg_ref, fg_ref, pack_ref, hidden_ref, *out_refs = refs
    rows = hidden_ref.shape[0]
    order = (tp_ref[0], 1 - tp_ref[0])[:sources]

    normed = []
    for n, t in enumerate(order):
        span = pl.ds(pl.multiple_of(t * rows, rows), rows)
        mixed = dot(own_ref[span, :], w_own[...]) + dot(other_ref[span, :], w_other[...])
        hidden = (resid_refs[n][...].astype(F32) + rms(mixed, pg_ref[...])).astype(BF16)
        if n == 0:
            hidden_ref[...] = hidden
        normed.append(rms(hidden.astype(F32), fg_ref[...]).astype(BF16))
    normed = jnp.concatenate(normed, axis=0)
    count = out_refs[0].shape[0]
    for n, ref in enumerate(out_refs):
        ref[...] = dot(pack_ref[n * count:(n + 1) * count, :], normed).astype(BF16)


def project(tp_index, own, other, w_own, w_other, resids, post_gain, ffn_gain, pack, pieces):
    rows, width = resids[0].shape
    count = pack.shape[0] // pieces
    vmem = pl.BlockSpec(memory_space=pltpu.VMEM)
    return pl.pallas_call(
        functools.partial(project_kernel, sources=len(resids)),
        in_specs=[pl.BlockSpec(memory_space=pltpu.SMEM)] + [vmem] * (7 + len(resids)),
        out_specs=(vmem,) * (1 + pieces),
        out_shape=(jax.ShapeDtypeStruct((rows, width), BF16),)
        + (jax.ShapeDtypeStruct((count, width), BF16),) * pieces,
        compiler_params=params(24),
        name="project",
    )(tp_index, own, other, w_own, w_other, *resids, post_gain[None, :], ffn_gain[None, :], pack)


def load_kernel(after_ref, *refs):
    count = (len(refs) - 1) // 2
    sources, targets, sem = refs[:count], refs[count:-1], refs[-1]
    copies = [
        pltpu.make_async_copy(source.at[0], target, sem.at[n])
        for n, (source, target) in enumerate(zip(sources, targets))
    ]
    for copy in copies:
        copy.start()
    for copy in copies:
        copy.wait()


def load(after, weights):
    hbm = pl.BlockSpec(memory_space=pltpu.HBM)
    vmem = pl.BlockSpec(memory_space=pltpu.VMEM)
    weights = [pltpu.with_memory_space_constraint(w, pltpu.HBM) for w in weights]
    return pl.pallas_call(
        load_kernel,
        in_specs=[hbm] * (1 + len(weights)),
        out_specs=(vmem,) * len(weights),
        out_shape=tuple(pltpu.VMEM(w.shape[1:], BF16) for w in weights),
        scratch_shapes=[pltpu.SemaphoreType.DMA((len(weights),))],
        compiler_params=params(1),
        cost_estimate=pl.CostEstimate(flops=10 ** 10, bytes_accessed=12 * weights[0].size, transcendentals=0),
        name="load",
    )(after, *weights)


def expert_kernel(*refs, pieces, block, out_block, fetch):
    x_refs, refs = refs[:pieces], refs[pieces:]
    gate_refs, up_refs, down_refs, refs = refs[0:2], refs[2:4], refs[4:6], refs[6:]
    y_refs, refs = refs[:pieces], refs[pieces:]
    copies = ()
    if fetch:
        down_hbm, down_refs, sem, refs = down_refs, refs[:2], refs[-1], refs[2:-1]
        copies = [pltpu.make_async_copy(down_hbm[n].at[0], down_refs[n], sem.at[n]) for n in range(2)]
    for copy in copies:
        copy.start()
    x_ref, inner_ref = refs
    width, hidden = gate_refs[0].shape
    count = x_refs[0].shape[0]
    for n, ref in enumerate(x_refs):
        x_ref[n * count:(n + 1) * count, :] = ref[...]

    for half in range(2):

        def rise(i, carry, half=half):
            at = pl.ds(pl.multiple_of(i * block, block), block)
            x = x_ref[...]
            gate = dot(x, gate_refs[half][:, at])
            up = dot(x, up_refs[half][:, at])
            inner_ref[half, :, at] = (gate / (1.0 + jnp.exp(-gate)) * up).astype(BF16)
            return carry

        lax.fori_loop(0, hidden // block, rise, 0, unroll=x_ref.shape[0] <= 192)

    for copy in copies:
        copy.wait()

    def fall(i, carry):
        at = pl.ds(pl.multiple_of(i * out_block, out_block), out_block)
        total = None
        for half in range(2):
            part = dot(inner_ref[half], down_refs[half][:, at]).astype(BF16).astype(F32)
            total = part if total is None else total + part
        total = total.astype(BF16)
        for n, ref in enumerate(y_refs):
            ref[:, at] = total[n * count:(n + 1) * count, :]
        return carry

    lax.fori_loop(0, width // out_block, fall, 0, unroll=x_ref.shape[0] <= 192)


def expert(pieces, rises, falls, fetch):
    count, width = pieces[0].shape
    rows = count * len(pieces)
    hidden = rises[0].shape[1]
    vmem = pl.BlockSpec(memory_space=pltpu.VMEM)
    hbm = pl.BlockSpec(memory_space=pltpu.HBM)
    rises = [pltpu.with_memory_space_constraint(w, pltpu.VMEM) for w in rises]
    falls = [pltpu.with_memory_space_constraint(w, pltpu.HBM if fetch else pltpu.VMEM) for w in falls]
    kept = tuple(pltpu.VMEM((hidden, width), BF16) for _ in falls) if fetch else ()
    out = pl.pallas_call(
        functools.partial(
            expert_kernel,
            pieces=len(pieces),
            block=256 if hidden % 256 == 0 else 128,
            out_block=512 if width % 512 == 0 else 128,
            fetch=fetch,
        ),
        in_specs=[vmem] * (len(pieces) + len(rises)) + [hbm if fetch else vmem] * 2,
        out_specs=(vmem,) * (len(pieces) + len(kept)),
        out_shape=(jax.ShapeDtypeStruct((count, width), BF16),) * len(pieces) + kept,
        scratch_shapes=[pltpu.VMEM((rows, width), BF16), pltpu.VMEM((2, rows, hidden), BF16)]
        + ([pltpu.SemaphoreType.DMA((2,))] if fetch else []),
        compiler_params=params(max(8, rows // 24)),
        cost_estimate=pl.CostEstimate(
            flops=12 * rows * width * hidden, bytes_accessed=8 * rows * width, transcendentals=2 * rows * hidden
        ),
        name="expert",
    )(*pieces, *rises, *falls)
    return out[:len(pieces)], out[len(pieces):]


def gather_kernel(*refs, pieces, source):
    back_refs, (pick_ref, weight_ref, out_ref, back_ref) = refs[:pieces], refs[pieces:]
    count, rows = back_refs[0].shape[0], out_ref.shape[0]
    span = slice(source * rows, (source + 1) * rows)
    for n, ref in enumerate(back_refs):
        back_ref[n * count:(n + 1) * count, :] = ref[...]
    combined = None
    for k in range(pick_ref.shape[0]):
        part = dot(pick_ref[k, span, :], back_ref[...]) * weight_ref[span, k:k + 1]
        combined = part if combined is None else combined + part
    out_ref[...] = combined.astype(out_ref.dtype)


def gather(back, pick, weight, source, dtype):
    rows, width = weight.shape[0] // 2, back[0].shape[1]
    vmem = pl.BlockSpec(memory_space=pltpu.VMEM)
    return pl.pallas_call(
        functools.partial(gather_kernel, pieces=len(back), source=source),
        in_specs=[vmem] * (len(back) + 2),
        out_specs=vmem,
        out_shape=jax.ShapeDtypeStruct((rows, width), dtype),
        scratch_shapes=[pltpu.VMEM((pick.shape[2], width), BF16)],
        compiler_params=params(20),
        cost_estimate=pl.CostEstimate(flops=10 ** 9, bytes_accessed=4 * rows * width, transcendentals=0),
        name="gather",
    )(*back, pick, weight)


def finish_kernel(own_ref, other_ref, hidden_ref, gain_ref, out_ref):
    combined = own_ref[...] + other_ref[...].astype(F32)
    out_ref[...] = (hidden_ref[...].astype(F32) + rms(combined, gain_ref[...])).astype(BF16)


def finish(own, other, hidden, gain):
    return pl.pallas_call(
        finish_kernel,
        out_shape=jax.ShapeDtypeStruct(own.shape, BF16),
        compiler_params=params(16),
        name="finish",
    )(own, other, hidden, gain[None, :])


def combine_kernel(back_ref, pick_ref, weight_ref, hidden_ref, gain_ref, out_ref):
    combined = None
    for k in range(pick_ref.shape[0]):
        part = dot(pick_ref[k], back_ref[...]) * weight_ref[:, k:k + 1]
        combined = part if combined is None else combined + part
    out_ref[...] = (hidden_ref[...].astype(F32) + rms(combined, gain_ref[...])).astype(BF16)


def combine(back, pick, weight, hidden, gain):
    return pl.pallas_call(
        combine_kernel,
        out_shape=jax.ShapeDtypeStruct(hidden.shape, BF16),
        compiler_params=params(16),
        name="combine",
    )(back, pick, weight, hidden, gain[None, :])


def swap_tp(x):
    count = lax.axis_size("tp")
    return lax.ppermute(x, "tp", [(i, (i + 1) % count) for i in range(count)])


def move(x, perm):
    return lax.ppermute(x, "sp", perm)


def per_device(
    queries,
    keys,
    values,
    q_gain,
    k_gain,
    resid,
    out_weight,
    post_gain,
    ffn_gain,
    post_ffn_gain,
    gate_w,
    up_w,
    down_w,
    route_ids,
    route_w,
):
    tok_local = queries.shape[0]
    width = resid.shape[1]
    tp_count = lax.axis_size("tp")
    sp_count = lax.axis_size("sp")
    top_count = route_ids.shape[1]
    expert_count = gate_w.shape[0] * sp_count
    capacity = 3 * tok_local * top_count // (2 * tp_count * expert_count)
    slots = expert_count * capacity

    tp_index = lax.axis_index("tp").astype(jnp.int32).reshape(1)
    sp_index = lax.axis_index("sp").astype(jnp.int32).reshape(1)
    paired = tp_count == 2 and expert_count == sp_count == 16 and capacity % 8 == 0

    qn, kv = prep(queries, keys, values, q_gain, k_gain)

    far = 4
    plane = sp_count // far

    def over_z(d):
        return move(kv, [(i, (i // plane ^ d) * plane + i % plane) for i in range(sp_count)])

    def in_plane(x):
        out = []
        for d in range(1, plane):
            out.append(move(x, [(i, i ^ d) for i in range(sp_count)]))
        return out

    z_blocks = [over_z(d) for d in range(1, far)]
    early = [kv, z_blocks[0]] + in_plane(kv) + in_plane(z_blocks[0])
    early += z_blocks[1:]
    late = in_plane(jnp.concatenate(z_blocks[1:], axis=0))

    ids, shares, resids = [route_ids.T], [route_w.T], [resid]
    if paired:
        ids.append(swap_tp(ids[0]))
        shares.append(swap_tp(shares[0]))
        resids.append(swap_tp(resid))
    w_other = swap_tp(out_weight)
    gates = (gate_w, swap_tp(gate_w))
    ups = (up_w, swap_tp(up_w))
    downs = (down_w, swap_tp(down_w))
    pick, weight, pack = route(ids + shares, jnp.concatenate([sp_index, tp_index]), expert_count, capacity)

    carry = attend(qn, early, None, False)
    attended = attend(qn, late, carry, True)
    hidden, *outgoing = project(
        tp_index,
        attended,
        swap_tp(attended),
        out_weight,
        w_other,
        resids,
        post_gain,
        ffn_gain,
        pack,
        sp_count // 2 if paired else 1,
    )
    loaded = load(hidden, gates + ups + (() if paired else downs))
    if not paired:
        swap_all = lambda x: lax.all_to_all(
            x.reshape(expert_count, capacity, width), "sp", split_axis=0, concat_axis=0, tiled=True
        ).reshape(slots, width)
        returned = swap_all(expert([swap_all(outgoing[0])], loaded[:4], loaded[4:], False)[0][0])
        return combine(returned, pick, weight, hidden, post_ffn_gain)

    def move_pair(x, j):
        perm = [(2 * i + t, 2 * (i ^ (2 * j + t)) + t) for i in range(sp_count) for t in range(2)]
        return lax.ppermute(x, ("sp", "tp"), perm)

    stages = ((6, 5, 3, 0), (7, 4, 2, 1))
    arrived = []
    for n, stage in enumerate(stages):
        arrived.append([])
        for j in stage:
            arrived[n].append(move_pair(outgoing[j], j))
    returned = [None] * len(outgoing)
    done = None
    for n, (stage, pieces) in enumerate(zip(stages, arrived)):
        if done is not None:
            pieces, _ = lax.optimization_barrier((pieces, done))
        done, kept = expert(pieces, loaded, downs, n == 0)
        downs = kept or downs
        for j, piece in zip(stage, done):
            returned[j] = move_pair(piece, j)
    from_other = swap_tp(gather(returned, pick, weight, 1, BF16))
    combined = gather(returned, pick, weight, 0, F32)
    return finish(combined, from_other, hidden, post_ffn_gain)


def solution(mesh):
    in_specs = (
        P("sp", "tp"),
        P("sp", "tp"),
        P("sp", "tp"),
        P(),
        P(),
        P(("sp", "tp"), None),
        P("tp", None),
        P(),
        P(),
        P(),
        P("sp", None, "tp"),
        P("sp", None, "tp"),
        P("sp", "tp", None),
        P(("sp", "tp"), None),
        P(("sp", "tp"), None),
    )
    out_specs = P(("sp", "tp"), None)
    return jax.shard_map(
        per_device, mesh=mesh, in_specs=in_specs, out_specs=out_specs, check_vma=False
    )
```
